32 devices in a mesh: sp: 8 (over z, x), tp: 4 (over y, core).
Axes of the slice: x: 2, y: 2, z: 4, core: 2. Of those that a mesh axis runs over, the one named last changes fastest.
Arguments:
- cot_out: bfloat16 [2048, 2048], P('sp', 'tp'), may hold values from -6 to 6
- route_ids: int32 [2048, 2], P('sp'), may hold values from 0 to 7, all different within a row; in each aligned block of 256 rows (0 to 255, 256 to 511, ...) at most 96 rows name the same one
- route_weight: float32 [2048, 2], P('sp'), may hold values from 0.1 to 1
- expert_inputs: bfloat16 [8, 768, 2048], P('sp'), may hold values from -48 to 48
- w_gate: bfloat16 [8, 2048, 1024], P('sp', None, 'tp'), may hold values from -0.125 to 0.125
- w_up: bfloat16 [8, 2048, 1024], P('sp', None, 'tp'), may hold values from -0.125 to 0.125
- w_down: bfloat16 [8, 1024, 2048], P('sp', 'tp'), may hold values from -0.1875 to 0.1875
- w_proj: bfloat16 [2048, 2048], P('tp'), may hold values from -0.125 to 0.125
- conv_out: bfloat16 [2048, 2048], P('sp', 'tp'), may hold values from -6 to 6
- channel_norm_gain: float32 [2048], P('tp'), may hold values from 0.1 to 1.9
- taps: float32 [31, 2048], P(None, 'tp'), may hold values from -1 to 1
- value_pre: bfloat16 [2048, 2048], P('sp', 'tp'), may hold values from -6 to 6
- gate_pre: bfloat16 [2048, 2048], P('sp', 'tp'), may hold values from -6 to 6
Outputs:
- grad_gate_w: bfloat16 [8, 2048, 1024], P('sp', None, 'tp')
- grad_up_w: bfloat16 [8, 2048, 1024], P('sp', None, 'tp')
- grad_down_w: bfloat16 [8, 1024, 2048], P('sp', 'tp')
- grad_proj: float32 [2048, 2048], P(('tp', 'sp'))
- grad_value: bfloat16 [2048, 2048], P('sp', 'tp')
- grad_gate: bfloat16 [2048, 2048], P('sp', 'tp')
The draws below stay inside these ranges and needn't reach their ends.
Inputs may be any that keep to these rules, and one draw needn't show every extreme that they name: `route_ids`: among the tokens of one index of sp no expert is chosen more than 96 times, a bound that some block reaches; a token's experts differ.
All inputs are finite; a program needn't handle non-finite values.
Results may differ from the reference program's by a relative error of at most 0.012.
Values may be sent and summed in bfloat16 or wider, within the bound.
A program may use at most 128 MiB of HBM per device.

```python
import math
import jax
import jax.numpy as jnp
import numpy as np
from jax import lax

D = 2048
F = 1024
WIDTH = 31
TOP = 2
TOK_DEV = 256
EXPERTS = 8
CAP = 96
SLOTS = 768
TOKENS = 2048
N_SP = 8
N_TP = 4


def draw_expert_inputs(key, part):
    keys = jax.random.split(jax.random.fold_in(key, 11), 2)
    shape = (EXPERTS, SLOTS, D)
    base = jax.random.truncated_normal(keys[0], -6.0, 6.0, shape, jnp.float32)
    scales = jnp.exp(jax.random.uniform(keys[1], (EXPERTS, SLOTS, 1), jnp.float32, jnp.log(0.5), jnp.log(6.0)))
    values = scales * base
    return jnp.clip(values, -48.0, 48.0).astype(jnp.bfloat16)


def spiked(values, own_key, source, target, parts, factor):
    def block_of(position):
        return (jnp.arange(values.shape[position]) // (values.shape[position] // parts)).reshape((-1,) + (1,) * (values.ndim - 1 - position))

    near = jax.random.permutation(own_key, parts)[block_of(target)]
    second = (block_of(target) + parts // 2) % parts
    return jnp.where((block_of(source) == near) | (block_of(source) == second), factor * values, values)


def level_of(own_key, dims, pieces, least, top_value):
    def one(axis_at, blocks):
        draws = jax.random.uniform(jax.random.fold_in(jax.random.fold_in(own_key, 6), axis_at), (blocks,), jnp.float32, least / len(pieces), top_value / len(pieces))
        return jnp.repeat(jnp.exp(draws), dims[axis_at] // blocks).reshape((-1,) + (1,) * (len(dims) - axis_at - 1))

    gain = one(*pieces[0])
    for cut in pieces[1:]:
        gain = gain * one(*cut)
    return gain


def shared_out(stream_key, own, number, rows, count, top, reach, lean):
    ranking = jax.random.permutation(stream_key, count)
    heavy_load, usual = shares(count, rows * top, reach, lean, True), shares(count, rows * top, reach, lean, False)
    places = jnp.arange(count)

    def named(tallies, offset_by):
        used = int((tallies > 0).sum())
        fixed = max(1, used // 4)
        passed = fixed + (places - fixed + offset_by * (used - fixed)) % max(1, count - fixed)
        return jnp.zeros((count,), jnp.int32).at[ranking[jnp.where(places < fixed, places, passed)]].set(jnp.asarray(tallies, jnp.int32))

    tallies = jnp.where(number % 4 == 0, named(heavy_load, number // 4), named(usual, number - number // 4 - 1))
    mixed = jax.random.permutation(jax.random.fold_in(own, 3), count)
    source_of, sink = mixed[0:count // 2 * 2:2], mixed[1:count // 2 * 2:2]
    room = jnp.minimum(tallies[source_of] - 1, reach - tallies[sink]) // 2
    room = jnp.where((source_of == ranking[0]) | (sink == ranking[0]) | (tallies[sink] == 0), 0, jnp.maximum(room, 0))
    passed = jax.random.randint(jax.random.fold_in(own, 4), (count // 2,), 0, 1 << 20) % (room + 1)
    tallies = tallies.at[source_of].add(-passed).at[sink].add(passed)
    members = jnp.searchsorted(jnp.cumsum(tallies), jnp.arange(rows * top), side="right").astype(jnp.int32)
    table = members.reshape(top, rows).T
    table = table[jax.random.permutation(jax.random.fold_in(own, 1), rows)]
    offset_by = jax.random.randint(jax.random.fold_in(own, 2), (rows, 1), 0, top)
    return jnp.take_along_axis(table, (jnp.arange(top)[None, :] + offset_by) % top, axis=1)


def shares(amount, total, limit, lean, full):
    portions = [(1 << 20) // math.isqrt(grade ** lean) + 1 for grade in range(1, amount + 1)]
    largest = limit if full else min(limit, max(-(-total // amount), total * portions[0] // sum(portions)))
    least = 1 if total - largest >= amount - 1 else 0
    given, rest = [largest] + [least] * (amount - 1), total - largest - least * (amount - 1)
    while rest > 0:
        free = [i for i in range(1, amount) if given[i] < largest] or [i for i in range(1, amount) if given[i] < limit]
        whole, budget = sum([portions[i] for i in free]), rest
        for i in free:
            extra = min(limit - given[i], max(1, budget * portions[i] // whole), rest)
            given[i] = given[i] + extra
            rest = rest - extra
    return np.array(given)


def centred(key, dims, width, most, cuts=(), held_as=jnp.bfloat16):
    drawn = jax.random.normal(key, dims, jnp.float32) * width
    if len(cuts) > 0:
        drawn = level_of(key, dims, cuts, -0.22, 0.18) * drawn
    return jnp.clip(drawn, min=-most, max=most).astype(held_as)


def gaussian_with(key, shape, spread, reach, shards, heavy, held_as=jnp.bfloat16):
    drawn = spread * jax.random.normal(key, shape, jnp.float32)
    if shards:
        drawn = drawn * level_of(key, shape, shards, -0.22, 0.18)
    return jnp.clip(spiked(drawn, jax.random.fold_in(key, 3), *heavy), -reach, reach).astype(held_as)


def setup_inputs(seed: int = 0) -> dict:
    seeds = jax.random.split(jax.random.key(seed), 14)
    cot_out = gaussian_with(seeds[0], (TOKENS, D), 1.0, 6.0, ((0, 8), (1, 4)), (0, 1, 8, 2.0))
    route_ids_keys = jax.random.split(jax.random.fold_in(seeds[1], 1), TOKENS // TOK_DEV)
    route_ids_turns = jax.random.permutation(jax.random.fold_in(seeds[1], 3), TOKENS // TOK_DEV)
    route_ids = jax.vmap(lambda own, number: shared_out(jax.random.fold_in(seeds[1], 2), own, number, TOK_DEV, EXPERTS, TOP, CAP, 2))(route_ids_keys, route_ids_turns).reshape((TOKENS, TOP))
    route_weight = jnp.clip(jnp.exp(math.log(1.0) - 2.3025851 * jax.random.uniform(seeds[2], (TOKENS, TOP), jnp.float32) ** level_of(seeds[2], (TOKENS, TOP), ((0, 8),), -0.2, 0.2)), 0.1, 1.0)
    expert_inputs = draw_expert_inputs(jax.random.fold_in(seeds[13], 71), 0)
    w_gate = centred(seeds[4], (EXPERTS, D, F), D ** -0.5, 0.125, ((0, 8), (2, 4)))
    w_up = centred(seeds[5], (EXPERTS, D, F), D ** -0.5, 0.125, ((0, 8), (2, 4)))
    w_down = centred(seeds[6], (EXPERTS, F, D), F ** -0.5, 0.1875, ((0, 8), (1, 4)))
    w_proj = centred(seeds[7], (D, D), D ** -0.5, 0.125, ((0, 4),))
    conv_out = centred(seeds[8], (TOKENS, D), 1.0, 6.0, ((0, 8), (1, 4)))
    channel_norm_gain = jnp.clip(1.0 + 0.18 * jax.random.normal(seeds[9], (D,), jnp.float32), 0.1, 1.9)
    taps = centred(seeds[10], (WIDTH, D), WIDTH ** -0.5, 1.0, ((1, 4),), jnp.float32)
    value_pre = centred(seeds[11], (TOKENS, D), 1.0, 6.0, ((0, 8), (1, 4)))
    gate_pre = centred(seeds[12], (TOKENS, D), 1.5, 6.0, ((0, 8), (1, 4)))
    return dict(cot_out=cot_out, route_ids=route_ids, route_weight=route_weight, expert_inputs=expert_inputs, w_gate=w_gate, w_up=w_up, w_down=w_down, w_proj=w_proj, conv_out=conv_out, channel_norm_gain=channel_norm_gain, taps=taps, value_pre=value_pre, gate_pre=gate_pre)


clamp_limit = 7.0
swish_alpha = 1.702
norm_epsilon = 1e-05

def one_expert(operands):
    rows_in, rows_cot, gate_weight, up_weight, down_weight = operands
    gate_lin = jnp.dot(rows_in, gate_weight, preferred_element_type=jnp.float32)
    up_lin = jnp.dot(rows_in, up_weight, preferred_element_type=jnp.float32)
    gate_c = jnp.minimum(gate_lin, clamp_limit)
    up_c = jnp.clip(up_lin, -clamp_limit, clamp_limit)
    sig = jax.nn.sigmoid(swish_alpha * gate_c)
    act = ((up_c + 1.0) * gate_c * sig).astype(jnp.bfloat16)
    grad_down = jnp.dot(act.T, rows_cot, preferred_element_type=jnp.float32).astype(jnp.bfloat16)
    d_act = jnp.dot(rows_cot, down_weight.T, preferred_element_type=jnp.float32)
    up_open = ((up_lin > -clamp_limit) & (up_lin < clamp_limit)).astype(jnp.float32)
    gate_open = (gate_lin < clamp_limit).astype(jnp.float32)
    d_up = (d_act * gate_c * sig * up_open).astype(jnp.bfloat16)
    d_gate = (d_act * (up_c + 1.0) * (sig + swish_alpha * gate_c * sig * (1.0 - sig)) * gate_open).astype(jnp.bfloat16)
    grad_gate = jnp.dot(rows_in.T, d_gate, preferred_element_type=jnp.float32).astype(jnp.bfloat16)
    grad_up = jnp.dot(rows_in.T, d_up, preferred_element_type=jnp.float32).astype(jnp.bfloat16)
    blocks = F // N_TP
    gate_parts = jnp.einsum('snf,dnf->nsd', d_gate.reshape(SLOTS, N_TP, blocks).astype(jnp.float32), gate_weight.reshape(D, N_TP, blocks).astype(jnp.float32))
    up_parts = jnp.einsum('snf,dnf->nsd', d_up.reshape(SLOTS, N_TP, blocks).astype(jnp.float32), up_weight.reshape(D, N_TP, blocks).astype(jnp.float32))
    rounded = (gate_parts + up_parts).astype(jnp.bfloat16)
    rounded = lax.optimization_barrier(rounded)
    input_grad = lax.optimization_barrier(jnp.sum(rounded.astype(jnp.float32), axis=0)).astype(jnp.bfloat16)
    return (grad_gate, grad_up, grad_down, input_grad)

def reference(cot_out, route_ids, route_weight, expert_inputs, w_gate, w_up, w_down, w_proj, conv_out, channel_norm_gain, taps, value_pre, gate_pre):
    block_ids = route_ids.reshape(N_SP, TOK_DEV * TOP)
    expert_hot = (block_ids[:, :, None] == jnp.arange(EXPERTS, dtype=jnp.int32)[None, None, :]).astype(jnp.int32)
    earlier = lax.optimization_barrier(jnp.sum((jnp.cumsum(expert_hot, axis=1) - expert_hot) * expert_hot, axis=2))
    dest_slot = (jnp.arange(N_SP, dtype=jnp.int32)[:, None] * CAP + earlier).reshape(-1).astype(jnp.int32)
    expert_of = block_ids.reshape(-1).astype(jnp.int32)
    repeated = jnp.repeat(cot_out, TOP, axis=0).astype(jnp.float32)
    scaled = (route_weight.reshape(-1)[:, None] * repeated).astype(jnp.bfloat16)
    expert_cot = jnp.zeros((EXPERTS, SLOTS, D), jnp.bfloat16).at[expert_of, dest_slot].set(scaled)
    grad_gate_w, grad_up_w, grad_down_w, expert_grad = lax.map(one_expert, (expert_inputs, expert_cot, w_gate, w_up, w_down))
    picked = expert_grad[expert_of, dest_slot].astype(jnp.float32).reshape(TOKENS, TOP, D)
    mix_grad = (cot_out.astype(jnp.float32) + lax.optimization_barrier(jnp.sum(picked, axis=1))).astype(jnp.bfloat16)
    convolution_filter = conv_out.astype(jnp.float32)
    channel_mean = lax.optimization_barrier(jnp.mean(convolution_filter, axis=1, keepdims=True))
    var = lax.optimization_barrier(jnp.mean(convolution_filter * convolution_filter, axis=1, keepdims=True)) - channel_mean * channel_mean
    inverse_deviation = lax.rsqrt(var + norm_epsilon)
    normalized_input = (convolution_filter - channel_mean) * inverse_deviation
    normalized_output = normalized_input * channel_norm_gain[None, :]
    sig = jax.nn.sigmoid(normalized_output)
    act_conv = (normalized_output * sig).astype(jnp.bfloat16)
    grad_proj = jnp.dot(act_conv.T, mix_grad, preferred_element_type=jnp.float32)
    d_act_conv = jnp.dot(mix_grad, w_proj.T, preferred_element_type=jnp.float32)
    normalized_gradient = d_act_conv * sig * (1.0 + normalized_output * (1.0 - sig)) * channel_norm_gain[None, :]
    first_moment_mean = lax.optimization_barrier(jnp.mean(normalized_gradient, axis=1, keepdims=True))
    second_moment_mean = lax.optimization_barrier(jnp.mean(normalized_gradient * normalized_input, axis=1, keepdims=True))
    convolution_gradient = inverse_deviation * (normalized_gradient - first_moment_mean - normalized_input * second_moment_mean)
    extended = jnp.concatenate([convolution_gradient, jnp.zeros((WIDTH - 1, D), jnp.float32)], axis=0)
    d_glu = jnp.zeros((TOKENS, D), jnp.float32)
    for offset in range(WIDTH):
        begin = WIDTH - 1 - offset
        d_glu = d_glu + taps[offset][None, :] * extended[begin:begin + TOKENS]
    gate_sig = jax.nn.sigmoid(gate_pre.astype(jnp.float32))
    grad_value = (d_glu * gate_sig).astype(jnp.bfloat16)
    grad_gate = (d_glu * value_pre.astype(jnp.float32) * gate_sig * (1.0 - gate_sig)).astype(jnp.bfloat16)
    return (grad_gate_w, grad_up_w, grad_down_w, grad_proj, grad_value, grad_gate)
```

```python
import functools

import jax
import jax.numpy as jnp
from jax import lax
from jax.experimental import pallas as pl
from jax.experimental.pallas import tpu as pltpu
from jax.sharding import PartitionSpec as P

clamp_limit = 7.0
swish_alpha = 1.702
norm_epsilon = 1e-05
MESH = pl.DeviceIdType.MESH
VMEM = pltpu.VMEM


def lanes(index, width):
    return pl.ds(pl.multiple_of(index * width, width), width)


def places(group, narrow):
    me, t = lax.axis_index("sp"), lax.axis_index("tp")
    near = t + 1 - 2 * lax.rem(t, 2)
    far = lax.rem(t + narrow // 2, narrow)
    return me, t, near, far, lax.rem(near + narrow // 2, narrow)


def spread(pairs):
    return sorted(range(1, pairs), key=lambda o: abs(2 * o - pairs))


def around(me, group, sign):
    pairs = group // 2
    half, parity = me // 2, lax.rem(me, 2)
    across = [
        2 * lax.rem(half + pairs + sign * o, pairs) + (parity if side == 0 else 1 - parity)
        for o in spread(pairs)
        for side in range(2)
    ]
    return 2 * half + 1 - parity, across


def remote(src, dst, send, recv, sp, tp):
    return pltpu.make_async_remote_copy(
        src_ref=src, dst_ref=dst, send_sem=send, recv_sem=recv, device_id=(sp, tp), device_id_type=MESH
    )


def meet(peers):
    barrier = pltpu.get_barrier_semaphore()
    for sp, tp in peers:
        pl.semaphore_signal(barrier, inc=1, device_id=(sp, tp), device_id_type=MESH)
    pl.semaphore_wait(barrier, len(peers))


def dots(lhs, rhs, left, right):
    return lax.dot_general(lhs, rhs, (((left,), (right,)), ((), ())), preferred_element_type=jnp.float32)


def expert_kernel(
    group,
    narrow,
    cap,
    ids_hbm,
    weight_hbm,
    cot_hbm,
    conv_hbm,
    rows_hbm,
    gate_hbm,
    up_hbm,
    down_hbm,
    mix_ref,
    stats_ref,
    gate_out,
    up_out,
    down_out,
    ids_ref,
    weight_ref,
    cot_ref,
    conv_ref,
    in_ref,
    pair_w,
    down_ref,
    out_ref,
    cot_rows,
    act_ref,
    up_slope,
    gate_slope,
    delta,
    part,
    pair_buf,
    far_out,
    far_in,
    done,
    home,
    stat_ref,
    *sems,
):
    a_s, a_r, n_s, n_r, f_s, f_r, m_s, m_r, pn_s, pn_r, pf_s, pf_r, h_s, h_r, t_s, t_r, l_s = sems
    f32, bf16 = jnp.float32, jnp.bfloat16
    me, t, near, far, cross = places(group, narrow)
    partner, across = around(me, group, 1)
    arriving = around(me, group, -1)[1]
    sp_peers = [partner] + across
    peers = [(p, t) for p in sp_peers] + [(me, near), (me, far), (me, cross)]
    barrier = pltpu.get_barrier_semaphore()
    for sp, tp in peers:
        pl.semaphore_signal(barrier, inc=1, device_id=(sp, tp), device_id_type=MESH)

    tokens, width = cot_ref.shape
    slots, model = cot_rows.shape
    hidden = down_ref.shape[0]
    chosen = ids_ref.shape[1]
    loads = [
        pltpu.make_async_copy(s, d, l_s.at[k])
        for k, (s, d) in enumerate(
            [
                (ids_hbm, ids_ref),
                (weight_hbm, weight_ref),
                (cot_hbm, cot_ref),
                (conv_hbm, conv_ref),
                (rows_hbm, in_ref),
                (gate_hbm, pair_w.at[:, pl.ds(0, hidden)]),
                (up_hbm, pair_w.at[:, pl.ds(hidden, hidden)]),
                (down_hbm, down_ref),
            ]
        )
    ]
    for c in loads:
        c.start()
    for c in loads[:3]:
        c.wait()

    ids = ids_ref[...]
    lane = lax.broadcasted_iota(jnp.int32, (tokens, 128), 1)
    spread_ids = jnp.zeros((tokens, 128), f32)
    for k in range(chosen):
        spread_ids = jnp.where(lane == k, ids[:, k : k + 1].astype(f32), spread_ids)
    ids_rows = jnp.transpose(spread_ids)[:8].astype(jnp.int32)
    experts = -(-group // 8) * 8
    expert = lax.broadcasted_iota(jnp.int32, (experts, tokens), 0)
    hots = [ids_rows[k : k + 1] == expert for k in range(chosen)]
    hot = functools.reduce(jnp.logical_or, hots).astype(f32).astype(bf16)
    first = lax.broadcasted_iota(jnp.int32, (tokens, tokens), 0)
    second = lax.broadcasted_iota(jnp.int32, (tokens, tokens), 1)
    earlier = dots(hot, (first < second).astype(f32).astype(bf16), 1, 0)
    slot_row = lax.broadcasted_iota(jnp.int32, (slots, tokens), 0)
    picks = []
    outgoing = jnp.zeros((slots, width), f32)
    for k in range(chosen):
        slot = jnp.sum(jnp.where(hots[k], earlier, 0.0), axis=0, keepdims=True).astype(jnp.int32)
        dest = ids_rows[k : k + 1] * cap + slot
        pick = (slot_row == dest).astype(f32).astype(bf16)
        scaled = (weight_ref[:, k : k + 1] * cot_ref[...].astype(f32)).astype(bf16)
        outgoing = outgoing + dots(pick, scaled, 1, 0)
        picks.append(pick)
    out_ref[...] = outgoing.astype(bf16)
    pick_any = functools.reduce(jnp.add, picks)

    def block(s):
        return pl.ds(pl.multiple_of(s * cap, cap), cap)

    def spot(s, column):
        return cot_rows.at[block(s), lanes(column, width)]

    cot_rows[block(me), lanes(t, width)] = out_ref[block(me), :]
    pl.semaphore_wait(barrier, len(peers))

    def swap(s):
        return remote(out_ref.at[block(s)], spot(me, t), a_s.at[s], a_r.at[me], s, t)

    def to_far(s):
        return remote(spot(s, t), spot(s, t), f_s.at[s], f_r.at[s], me, far)

    def to_near(s):
        return remote(spot(s, t), spot(s, t), n_s.at[s], n_r.at[s], me, near)

    def onward(s):
        return remote(spot(s, far), spot(s, far), m_s.at[s], m_r.at[s], me, near)

    def part_near(s, k):
        column = near if k == 0 else cross
        return remote(
            part.at[block(s), lanes(column, width)],
            pair_buf.at[k, block(s)],
            pn_s.at[s, k],
            pn_r.at[s, k],
            me,
            near,
        )

    def part_far(s):
        return remote(far_out.at[block(s)], far_in.at[block(s)], pf_s.at[s], pf_r.at[s], me, far)

    def to_home(s):
        return remote(done.at[block(s)], home.at[block(me)], h_s.at[s], h_r.at[me], s, t)

    def from_home(s):
        return remote(done.at[block(s)], home.at[block(s)], h_s.at[s], h_r.at[s], s, t)

    def arrive(s):
        remote(out_ref.at[block(s)], spot(s, t), a_s.at[s], a_r.at[s], s, t).wait_recv()

    def fan(s):
        to_far(s).start()
        to_near(s).start()

    def relay(s):
        to_far(s).wait_recv()
        onward(s).start()

    def slopes(piece, pieces):
        count = slots // pieces
        span = pl.ds(piece * count, count)
        both = jnp.dot(in_ref[span, :], pair_w[...], preferred_element_type=f32)
        gate_lin, up_lin = both[:, :hidden], both[:, hidden:]
        gate_c = jnp.minimum(gate_lin, clamp_limit)
        up_c = jnp.clip(up_lin, -clamp_limit, clamp_limit)
        sigma = jax.nn.sigmoid(swish_alpha * gate_c)
        lift, gated = up_c + 1.0, gate_c * sigma
        act_ref[span, :] = (lift * gated).astype(bf16)
        up_open = (up_lin > -clamp_limit) & (up_lin < clamp_limit)
        up_slope[span, :] = jnp.where(up_open, gated, 0.0)
        slope = lift * (sigma + swish_alpha * gated * (1.0 - sigma))
        gate_slope[span, :] = jnp.where(gate_lin < clamp_limit, slope, 0.0)

    def compute(s, ready):
        rows = block(s)
        if not ready:
            remote(spot(s, near), spot(s, near), n_s.at[s], n_r.at[s], me, near).wait_recv()
            remote(spot(s, cross), spot(s, cross), m_s.at[s], m_r.at[s], me, near).wait_recv()
        d_act = dots(cot_rows[rows, :], down_ref[...], 1, 1)
        d_gate = (d_act * gate_slope[rows, :]).astype(bf16)
        d_up = (d_act * up_slope[rows, :]).astype(bf16)
        delta[rows, pl.ds(0, hidden)] = d_gate
        delta[rows, pl.ds(hidden, hidden)] = d_up
        cut = min(model, 1024)
        for j in range(model // cut):
            span = pl.ds(j * cut, cut)
            part[rows, span] = dots(delta[rows, :], pair_w[span, :], 1, 1).astype(bf16)
        part_near(s, 1).start()
        part_near(s, 0).start()

    def pair_up(s):
        rows = block(s)
        part_near(s, 1).wait_recv()
        pair = part[rows, lanes(far, width)].astype(f32) + pair_buf[1, rows].astype(f32)
        far_out[rows, :] = pair.astype(bf16)
        part_far(s).start()

    def finish(s, own):
        rows = block(s)
        part_near(s, 0).wait_recv()
        part_far(s).wait_recv()
        total = part[rows, lanes(t, width)].astype(f32)
        total = total + pair_buf[0, rows].astype(f32) + far_in[rows, :].astype(f32)
        if own:
            home[rows, :] = total.astype(bf16)
        else:
            done[rows, :] = total.astype(bf16)
            to_home(s).start()

    for s in across + [partner]:
        swap(s).start()
    fan(me)
    loads[3].wait()
    conv = conv_ref[...].astype(f32)
    sums = jnp.where(lane == 0, jnp.sum(conv, axis=1, keepdims=True), 0.0)
    sums = jnp.where(lane == 1, jnp.sum(conv * conv, axis=1, keepdims=True), sums)
    stat_ref[...] = jnp.transpose(sums)[:8]
    small = []
    for k, p in enumerate((near, far, cross)):
        c = remote(stat_ref, stats_ref.at[t], t_s.at[k], t_r.at[k], me, p)
        c.start()
        small.append(c)
    stats_ref[t] = stat_ref[...]
    for c in loads[4:]:
        c.wait()
    pieces = 4
    slopes(0, pieces)
    arrive(partner)
    fan(partner)
    relay(me)
    fill = [functools.partial(slopes, p, pieces) for p in range(1, pieces)]
    count = len(arriving)

    def at(k):
        return arriving[k]

    for i in range(count + 5):
        if i - 5 >= 0 and i - 5 < count:
            finish(at(i - 5), False)
        if 0 <= i - 3 < count:
            pair_up(at(i - 3))
        if 0 <= i - 2 < count:
            compute(at(i - 2), False)
        if i < count:
            arrive(at(i))
            fan(at(i))
        if i == 0:
            relay(partner)
        elif i - 1 < count:
            relay(at(i - 1))
        for _ in range(2 - i):
            fill.pop(0)()
        if i == count:
            compute(partner, False)
            compute(me, False)
        if i == count + 2:
            pair_up(partner)
            pair_up(me)
            down_out[...] = dots(act_ref[...], cot_rows[...], 0, 0).astype(bf16)
        if i == count + 3:
            gate_out[...] = dots(in_ref[...], delta[:, :hidden], 0, 0).astype(bf16)
        if i == count + 4:
            up_out[...] = dots(in_ref[...], delta[:, hidden:], 0, 0).astype(bf16)
    finish(partner, False)
    finish(me, True)
    for s in sp_peers:
        from_home(s).wait_recv()
    summed = dots(pick_any, home[...], 0, 0)
    mix_ref[...] = (cot_ref[...].astype(f32) + summed).astype(bf16)
    for s in [me] + sp_peers:
        to_far(s).wait_send()
        to_near(s).wait_send()
        onward(s).wait_send()
        part_near(s, 0).wait_send()
        part_near(s, 1).wait_send()
        part_far(s).wait_send()
    for s in sp_peers:
        swap(s).wait_send()
        to_home(s).wait_send()
    for c in small:
        c.wait_send()
        c.wait_recv()


def expert_pass(ids, weight, cot, conv, rows_in, gate_weight, up_weight, down_weight):
    group, narrow = lax.axis_size("sp"), lax.axis_size("tp")
    tokens, width = cot.shape
    slots, model = rows_in.shape
    hidden = down_weight.shape[0]
    cap = slots // group
    f32, bf16 = jnp.float32, jnp.bfloat16
    dma = pltpu.SemaphoreType.DMA
    rows = (slots, width)
    return pl.pallas_call(
        functools.partial(expert_kernel, group, narrow, cap),
        out_shape=(
            jax.ShapeDtypeStruct((tokens, width), bf16),
            jax.ShapeDtypeStruct((narrow, 8, tokens), f32),
            jax.ShapeDtypeStruct((model, hidden), bf16),
            jax.ShapeDtypeStruct((model, hidden), bf16),
            jax.ShapeDtypeStruct((hidden, model), bf16),
        ),
        in_specs=[pl.BlockSpec(memory_space=pl.ANY)] * 8,
        out_specs=[pl.BlockSpec(memory_space=VMEM)] * 5,
        scratch_shapes=[
            VMEM(ids.shape, ids.dtype),
            VMEM(weight.shape, weight.dtype),
            VMEM(cot.shape, bf16),
            VMEM(conv.shape, bf16),
            VMEM(rows_in.shape, bf16),
            VMEM((model, 2 * hidden), bf16),
            VMEM(down_weight.shape, bf16),
            VMEM(rows, bf16),
            VMEM((slots, model), bf16),
            VMEM((slots, hidden), bf16),
            VMEM((slots, hidden), f32),
            VMEM((slots, hidden), f32),
            VMEM((slots, 2 * hidden), bf16),
            VMEM((slots, model), bf16),
            VMEM((2,) + rows, bf16),
            VMEM(rows, bf16),
            VMEM(rows, bf16),
            VMEM(rows, bf16),
            VMEM(rows, bf16),
            VMEM((8, tokens), f32),
        ]
        + [dma((group,))] * 8
        + [dma((group, 2))] * 2
        + [dma((group,))] * 4
        + [dma((3,))] * 2
        + [dma((8,))],
        compiler_params=pltpu.CompilerParams(
            collective_id=0, has_side_effects=True, vmem_limit_bytes=60 * 1024 * 1024
        ),
    )(ids, weight, cot, conv, rows_in, gate_weight, up_weight, down_weight)


def widen_kernel(narrow, width, pieces, mix_ref, full_ref, *sems):
    n_s, n_r, f_s, f_r, m_s, m_r, l_s = sems
    me, t, near, far, cross = places(1, narrow)
    meet([(me, near), (me, far)])
    rows = mix_ref.shape[0] // pieces

    def src(k):
        return mix_ref.at[pl.ds(k * rows, rows)]

    def spot(k, column):
        return full_ref.at[pl.ds(k * rows, rows), lanes(column, width)]

    def to_far(k):
        return remote(src(k), spot(k, t), f_s.at[k], f_r.at[k], me, far)

    def to_near(k):
        return remote(src(k), spot(k, t), n_s.at[k], n_r.at[k], me, near)

    def onward(k):
        return remote(spot(k, far), spot(k, far), m_s.at[k], m_r.at[k], me, near)

    own = pltpu.make_async_copy(mix_ref, full_ref.at[:, lanes(t, width)], l_s.at[0])
    for k in range(pieces):
        to_far(k).start()
    for k in range(pieces):
        to_near(k).start()
    own.start()
    for k in range(pieces):
        to_far(k).wait_recv()
        onward(k).start()
    own.wait()
    for k in range(pieces):
        to_far(k).wait_send()
        to_near(k).wait()
        onward(k).wait()


def widen(mix):
    rows, width = mix.shape
    narrow = lax.axis_size("tp")
    pieces = 4
    dma = pltpu.SemaphoreType.DMA
    return pl.pallas_call(
        functools.partial(widen_kernel, narrow, width, pieces),
        out_shape=jax.ShapeDtypeStruct((rows, narrow * width), mix.dtype),
        in_specs=[pl.BlockSpec(memory_space=VMEM)],
        out_specs=pl.BlockSpec(memory_space=VMEM),
        scratch_shapes=[dma((pieces,))] * 6 + [dma((1,))],
        compiler_params=pltpu.CompilerParams(collective_id=2, has_side_effects=True),
    )(mix)


def tail_kernel(
    group,
    narrow,
    reach,
    parts_ref,
    grad_ref,
    hat_ref,
    stat_ref,
    taps_ref,
    proj_ref,
    others,
    glu_ref,
    stats,
    next_stats,
    next_grad,
    next_hat,
    extended,
    pair_in,
    pair_sum,
    *sems,
):
    t_s, t_r, v_s, v_r, h_s, h_r, x_s, x_r, z_s, z_r = sems
    f32 = jnp.float32
    me, t, near, far, cross = places(group, narrow)
    rows, cols = grad_ref.shape
    halo = next_grad.shape[0]
    pairs = group // 2
    parity = lax.rem(me, 2)
    half = me // 2
    partner = me + 1 - 2 * parity
    ahead, behind = lax.rem(me + 1, group), lax.rem(me + group - 1, group)
    siblings = [lax.rem(t + o, narrow) for o in range(1, narrow)]
    alike = [lax.rem(half + o, pairs) for o in spread(pairs)]
    cut = parts_ref.shape[2] // 2
    sides = [pl.ds(h * cut, cut) for h in range(2)]
    everyone = [t] + siblings
    meet(
        [(me, p) for p in siblings]
        + [(ahead, p) for p in everyone]
        + [(behind, p) for p in everyone]
        + [(partner, t)]
        + [(2 * q + parity, t) for q in alike]
    )
    sends = []
    for k, p in enumerate(siblings):
        sends.append(remote(stat_ref, stats.at[k], t_s.at[k], t_r.at[k], me, p))
    for k, p in enumerate(everyone):
        sends.append(remote(stat_ref, next_stats.at[k], v_s.at[k], v_r.at[k], behind, p))
    sends.append(remote(grad_ref.at[pl.ds(0, halo)], next_grad, h_s.at[0], h_r.at[0], behind, t))
    sends.append(remote(hat_ref.at[pl.ds(0, halo)], next_hat, h_s.at[1], h_r.at[1], behind, t))
    for c in sends:
        c.start()

    def swap(q, h):
        side = sides[h]
        return remote(
            parts_ref.at[2 * q + 1 - parity, :, side],
            pair_in.at[q, :, side],
            x_s.at[q, h],
            x_r.at[q, h],
            partner,
            t,
        )

    def passing(source, target, h):
        slot = others.at[slot_of(source, target), :, sides[h]]
        return slot, z_r.at[source, h]

    def scatter(q, h):
        slot, arrival = passing(half, q, h)
        return remote(pair_sum.at[q, :, sides[h]], slot, z_s.at[q, h], arrival, 2 * q + parity, t)

    def slot_of(source, target):
        return lax.rem(target - source + pairs, pairs) - 1

    order = alike + [half]
    for q in order:
        for h in range(2):
            swap(q, h).start()
    for c in sends:
        c.wait_recv()

    channels = cols * narrow

    def finished(grad, hat, total, own):
        total = jnp.transpose(total)
        deviation = jnp.transpose(own)[:, 2:3]
        count = grad.shape[0]
        first, second = total[:count, 0:1] / channels, total[:count, 1:2] / channels
        return deviation[:count] * (grad - first - hat * second)

    total = stat_ref[...]
    following = next_stats[0]
    for k in range(narrow - 1):
        total = total + stats[k]
        following = following + next_stats[k + 1]
    extended[pl.ds(0, rows), :] = finished(grad_ref[...], hat_ref[...], total, stat_ref[...])
    beyond = finished(next_grad[...], next_hat[...], following, next_stats[0])
    extended[pl.ds(rows, halo), :] = jnp.where(me == group - 1, jnp.zeros_like(beyond), beyond)

    step = 32
    strips = cols // 128

    def convolve(index, carry):
        start = pl.multiple_of((index // strips) * step, step)
        column = lanes(lax.rem(index, strips), 128)
        total = jnp.zeros((step, 128), f32)
        window = extended[pl.ds(start, step + halo), column]
        for turn in range(8):
            shifted = window if turn == 0 else pltpu.roll(window, step + halo - turn, 0)
            for j in range(turn, reach, 8):
                total = total + taps_ref[reach - 1 - j : reach - j, column] * shifted[j - turn : j - turn + step]
        glu_ref[pl.ds(start, step), column] = total
        return carry

    turns = rows // step * strips
    marks = [turns * i // (2 * pairs) for i in range(2 * pairs + 1)]
    for i, q in enumerate(order):
        for h in range(2):
            lax.fori_loop(marks[2 * i + h], marks[2 * i + h + 1], convolve, 0)
            swap(q, h).wait_recv()
            both = parts_ref[2 * q + parity, :, sides[h]].astype(f32) + pair_in[q, :, sides[h]].astype(f32)
            if i < pairs - 1:
                pair_sum[q, :, sides[h]] = both.astype(pair_sum.dtype)
                scatter(q, h).start()
            else:
                proj_ref[:, sides[h]] = both
    for q in alike:
        for h in range(2):
            slot, arrival = passing(q, half, h)
            remote(pair_sum.at[q, :, sides[h]], slot, z_s.at[q, h], arrival, 2 * q + parity, t).wait_recv()
    for c in sends:
        c.wait_send()
    for h in range(2):
        for q in order:
            swap(q, h).wait_send()
        for q in alike:
            scatter(q, h).wait_send()


def tail(parts, grad, hat, stat, taps):
    group, block, model = parts.shape
    rows, cols = grad.shape
    narrow = lax.axis_size("tp")
    reach = taps.shape[0]
    halo = -(-(reach - 1) // 8) * 8
    pairs = group // 2
    f32 = jnp.float32
    dma = pltpu.SemaphoreType.DMA
    return pl.pallas_call(
        functools.partial(tail_kernel, group, narrow, reach),
        out_shape=(
            jax.ShapeDtypeStruct((block, model), f32),
            jax.ShapeDtypeStruct((pairs - 1, block, model), parts.dtype),
            jax.ShapeDtypeStruct((rows, cols), f32),
        ),
        in_specs=[pl.BlockSpec(memory_space=VMEM)] * 5,
        out_specs=[pl.BlockSpec(memory_space=VMEM)] * 3,
        scratch_shapes=[
            VMEM((narrow - 1,) + stat.shape, f32),
            VMEM((narrow,) + stat.shape, f32),
            VMEM((halo, cols), f32),
            VMEM((halo, cols), f32),
            VMEM((rows + halo, cols), f32),
            VMEM((pairs, block, model), parts.dtype),
            VMEM((pairs, block, model), parts.dtype),
            dma((narrow - 1,)),
            dma((narrow - 1,)),
            dma((narrow,)),
            dma((narrow,)),
            dma((2,)),
            dma((2,)),
        ]
        + [dma((pairs, 2))] * 4,
        compiler_params=pltpu.CompilerParams(collective_id=3, has_side_effects=True),
    )(parts, grad, hat, stat, taps)


def per_device(
    cot_out,
    route_ids,
    route_weight,
    expert_inputs,
    w_gate,
    w_up,
    w_down,
    w_proj,
    conv_out,
    channel_norm_gain,
    taps,
    value_pre,
    gate_pre,
):
    group_size = lax.axis_size("sp")
    narrow_size = lax.axis_size("tp")
    tok_rows, local_cols = cot_out.shape
    f32, bf16 = jnp.float32, jnp.bfloat16
    convolution_filter = conv_out.astype(f32)
    rows_in = expert_inputs[0]
    slot_rows, model_width = rows_in.shape
    capacity = slot_rows // group_size
    fitted = -(-capacity // 16) * 16
    if fitted != capacity:
        rows_in = rows_in.reshape(group_size, capacity, model_width)
        rows_in = jnp.pad(rows_in, ((0, 0), (0, fitted - capacity), (0, 0)))
        rows_in = rows_in.reshape(group_size * fitted, model_width)
    mix_grad, stats, grad_gate_part, grad_up_part, grad_down = expert_pass(
        route_ids, route_weight, cot_out, conv_out, rows_in, w_gate[0], w_up[0], w_down[0]
    )
    mix_full = widen(mix_grad)
    channel_total = local_cols * narrow_size
    first_sum, square_sum = jnp.sum(stats, axis=0)[:2]
    channel_mean = (first_sum / channel_total)[:, None]
    var = (square_sum / channel_total)[:, None] - channel_mean * channel_mean
    inverse_deviation = lax.rsqrt(var + norm_epsilon)
    normalized_input = (convolution_filter - channel_mean) * inverse_deviation
    normalized_output = normalized_input * channel_norm_gain[None, :]
    sigma_conv = jax.nn.sigmoid(normalized_output)
    act_conv = (normalized_output * sigma_conv).astype(bf16)
    partial_proj = lax.dot_general(
        act_conv, mix_full, (((0,), (0,)), ((), ())), preferred_element_type=f32
    ).astype(bf16)
    d_act_conv = jnp.dot(mix_full, w_proj.T, preferred_element_type=f32)
    normalized_gradient = (
        d_act_conv
        * sigma_conv
        * (1.0 + normalized_output * (1.0 - sigma_conv))
        * channel_norm_gain[None, :]
    )
    terms = jnp.stack(
        [
            jnp.sum(normalized_gradient, axis=1),
            jnp.sum(normalized_gradient * normalized_input, axis=1),
            inverse_deviation[:, 0],
        ]
    )
    terms = jnp.pad(terms, ((0, 8 - terms.shape[0]), (0, 0)))
    own_proj, other_proj, d_glu = tail(
        partial_proj.reshape(group_size, local_cols // group_size, model_width),
        normalized_gradient,
        normalized_input,
        terms,
        taps,
    )
    grad_proj = own_proj + jnp.sum(other_proj.astype(f32), axis=0)
    gate_sig = jax.nn.sigmoid(gate_pre.astype(f32))
    grad_value = (d_glu * gate_sig).astype(bf16)
    grad_gate = (d_glu * value_pre.astype(f32) * gate_sig * (1.0 - gate_sig)).astype(bf16)
    return (
        grad_gate_part[None],
        grad_up_part[None],
        grad_down[None],
        grad_proj,
        grad_value,
        grad_gate,
    )


def solution(mesh):
    return jax.shard_map(
        per_device,
        mesh=mesh,
        in_specs=(
            P("sp", "tp"),
            P("sp", None),
            P("sp", None),
            P("sp", None, None),
            P("sp", None, "tp"),
            P("sp", None, "tp"),
            P("sp", "tp", None),
            P("tp", None),
            P("sp", "tp"),
            P("tp"),
            P(None, "tp"),
            P("sp", "tp"),
            P("sp", "tp"),
        ),
        out_specs=(
            P("sp", None, "tp"),
            P("sp", None, "tp"),
            P("sp", "tp", None),
            P(("tp", "sp"), None),
            P("sp", "tp"),
            P("sp", "tp"),
        ),
        check_vma=False,
    )
```

```python
import functools

import jax
import jax.numpy as jnp
from jax import lax
from jax.experimental import pallas as pl
from jax.experimental.pallas import tpu as pltpu
from jax.sharding import PartitionSpec as P

clamp_limit = 7.0
swish_alpha = 1.702
norm_epsilon = 1e-05
MESH = pl.DeviceIdType.MESH
VMEM = pltpu.VMEM


def lanes(index, width):
    return pl.ds(pl.multiple_of(index * width, width), width)


def places(group, narrow):
    me, t = lax.axis_index("sp"), lax.axis_index("tp")
    near = t + 1 - 2 * lax.rem(t, 2)
    far = lax.rem(t + narrow // 2, narrow)
    return me, t, near, far, lax.rem(near + narrow // 2, narrow)


def spread(pairs):
    return sorted(range(1, pairs), key=lambda o: abs(2 * o - pairs))


def around(me, group, sign):
    pairs = group // 2
    half, parity = me // 2, lax.rem(me, 2)
    across = [
        2 * lax.rem(half + pairs + sign * o, pairs) + (parity if side == 0 else 1 - parity)
        for o in spread(pairs)
        for side in range(2)
    ]
    return 2 * half + 1 - parity, across


def remote(src, dst, send, recv, sp, tp):
    return pltpu.make_async_remote_copy(
        src_ref=src, dst_ref=dst, send_sem=send, recv_sem=recv, device_id=(sp, tp), device_id_type=MESH
    )


def meet(peers):
    barrier = pltpu.get_barrier_semaphore()
    for sp, tp in peers:
        pl.semaphore_signal(barrier, inc=1, device_id=(sp, tp), device_id_type=MESH)
    pl.semaphore_wait(barrier, len(peers))


def dots(lhs, rhs, left, right):
    return lax.dot_general(lhs, rhs, (((left,), (right,)), ((), ())), preferred_element_type=jnp.float32)


small_loads = ("ids", "weight", "cot", "conv", "gain")


def whole_kernel(group, narrow, cap, inputs, results, names, *refs):
    r = dict(zip(names, refs[inputs + results :]))
    r["result"] = refs[inputs : inputs + results]
    ids_ref, weight_ref, cot_ref, conv_ref, gain_ref = (r[n] for n in small_loads)
    in_ref, pair_w, down_ref, w_ref, taps_ref = r["in"], r["pair_w"], r["down"], r["proj"], r["taps"]
    out_ref, cot_rows, act_ref, delta, part = r["out"], r["cot_rows"], r["act"], r["delta"], r["part"]
    up_slope, gate_slope, pair_buf = r["up_slope"], r["gate_slope"], r["pair_buf"]
    far_out, far_in, done, home = r["far_out"], r["far_in"], r["done"], r["home"]
    stat_ref, stats_ref, term_ref, terms_ref = r["stat"], r["stats"], r["term"], r["terms"]
    mix_full, parts, pair_in, pair_sum = r["mix_full"], r["parts"], r["pair_in"], r["pair_sum"]
    others, own_sum, extended, beyond = r["others"], r["own_sum"], r["extended"], r["beyond"]
    conv_act, hat_ref, slope_ref, dev_ref = r["conv_act"], r["hat"], r["slope"], r["dev"]
    a_s, a_r, n_s, n_r, f_s, f_r, m_s, m_r = (r[n] for n in ("a_s", "a_r", "n_s", "n_r", "f_s", "f_r", "m_s", "m_r"))
    pn_s, pn_r, pf_s, pf_r, h_s, h_r = (r[n] for n in ("pn_s", "pn_r", "pf_s", "pf_r", "h_s", "h_r"))
    t_s, t_r, u_s, u_r, l_s, o_s = (r[n] for n in ("t_s", "t_r", "u_s", "u_r", "l_s", "o_s"))
    wn_s, wn_r, wf_s, wf_r, wm_s, wm_r = (r[n] for n in ("wn_s", "wn_r", "wf_s", "wf_r", "wm_s", "wm_r"))
    x_s, x_r, z_s, z_r, e_s, e_r = (r[n] for n in ("x_s", "x_r", "z_s", "z_r", "e_s", "e_r"))
    f32, bf16 = jnp.float32, jnp.bfloat16
    me, t, near, far, cross = places(group, narrow)
    partner, across = around(me, group, 1)
    arriving = around(me, group, -1)[1]
    sp_peers = [partner] + across
    peers = [(p, t) for p in sp_peers] + [(me, near), (me, far), (me, cross)]
    barrier = pltpu.get_barrier_semaphore()
    for sp, tp in peers:
        pl.semaphore_signal(barrier, inc=1, device_id=(sp, tp), device_id_type=MESH)

    tokens, width = cot_ref.shape
    slots, model = cot_rows.shape
    hidden = down_ref.shape[0]
    chosen = ids_ref.shape[0]
    channels = width * narrow
    targets = [ids_ref, weight_ref, cot_ref, conv_ref, gain_ref, in_ref]
    targets += [pair_w.at[:, pl.ds(0, hidden)], pair_w.at[:, pl.ds(hidden, hidden)], down_ref]
    targets += [w_ref, taps_ref, r["value"], r["gate"]]
    loads = [pltpu.make_async_copy(refs[k], d, l_s.at[k]) for k, d in enumerate(targets)]
    for c in loads:
        c.start()
    for c in loads[:3]:
        c.wait()

    ids_rows = ids_ref[...]
    lane = lax.broadcasted_iota(jnp.int32, (tokens, 128), 1)
    row = lax.broadcasted_iota(jnp.int32, (8, tokens), 0)
    weight_rows = jnp.zeros((8, tokens), f32)
    for k in range(chosen):
        weight_rows = jnp.where(row == k, weight_ref[k : k + 1, :], weight_rows)
    weights = jnp.transpose(weight_rows)
    experts = -(-group // 8) * 8
    expert = lax.broadcasted_iota(jnp.int32, (experts, tokens), 0)
    hots = [ids_rows[k : k + 1] == expert for k in range(chosen)]
    hot = functools.reduce(jnp.logical_or, hots).astype(f32).astype(bf16)
    first = lax.broadcasted_iota(jnp.int32, (tokens, tokens), 0)
    second = lax.broadcasted_iota(jnp.int32, (tokens, tokens), 1)
    earlier = dots(hot, (first < second).astype(f32).astype(bf16), 1, 0)
    slot_row = lax.broadcasted_iota(jnp.int32, (slots, tokens), 0)
    picks = []
    outgoing = jnp.zeros((slots, width), f32)
    for k in range(chosen):
        slot = jnp.sum(jnp.where(hots[k], earlier, 0.0), axis=0, keepdims=True).astype(jnp.int32)
        dest = ids_rows[k : k + 1] * cap + slot
        pick = (slot_row == dest).astype(f32).astype(bf16)
        scaled = (weights[:, k : k + 1] * cot_ref[...].astype(f32)).astype(bf16)
        outgoing = outgoing + dots(pick, scaled, 1, 0)
        picks.append(pick)
    out_ref[...] = outgoing.astype(bf16)
    pick_any = functools.reduce(jnp.add, picks)

    def block(s):
        return pl.ds(pl.multiple_of(s * cap, cap), cap)

    def spot(s, column):
        return cot_rows.at[block(s), lanes(column, width)]

    cot_rows[block(me), lanes(t, width)] = out_ref[block(me), :]
    pl.semaphore_wait(barrier, len(peers))

    def swap(s):
        return remote(out_ref.at[block(s)], spot(me, t), a_s.at[s], a_r.at[me], s, t)

    def to_far(s):
        return remote(spot(s, t), spot(s, t), f_s.at[s], f_r.at[s], me, far)

    def to_near(s):
        return remote(spot(s, t), spot(s, t), n_s.at[s], n_r.at[s], me, near)

    def onward(s):
        return remote(spot(s, far), spot(s, far), m_s.at[s], m_r.at[s], me, near)

    def part_near(s, k):
        column = near if k == 0 else cross
        return remote(
            part.at[block(s), lanes(column, width)],
            pair_buf.at[k, block(s)],
            pn_s.at[s, k],
            pn_r.at[s, k],
            me,
            near,
        )

    def part_far(s):
        return remote(far_out.at[block(s)], far_in.at[block(s)], pf_s.at[s], pf_r.at[s], me, far)

    def to_home(s):
        return remote(done.at[block(s)], home.at[block(me)], h_s.at[s], h_r.at[me], s, t)

    def from_home(s):
        return remote(done.at[block(s)], home.at[block(s)], h_s.at[s], h_r.at[s], s, t)

    def arrive(s):
        remote(out_ref.at[block(s)], spot(s, t), a_s.at[s], a_r.at[s], s, t).wait_recv()

    def fan(s):
        to_far(s).start()
        to_near(s).start()

    def relay(s):
        to_far(s).wait_recv()
        onward(s).start()

    def slopes(piece, pieces):
        count = slots // pieces
        span = pl.ds(piece * count, count)
        both = jnp.dot(in_ref[span, :], pair_w[...], preferred_element_type=f32)
        gate_lin, up_lin = both[:, :hidden], both[:, hidden:]
        gate_c = jnp.minimum(gate_lin, clamp_limit)
        up_c = jnp.clip(up_lin, -clamp_limit, clamp_limit)
        sigma = jax.nn.sigmoid(swish_alpha * gate_c)
        lift, gated = up_c + 1.0, gate_c * sigma
        act_ref[span, :] = (lift * gated).astype(bf16)
        up_open = (up_lin > -clamp_limit) & (up_lin < clamp_limit)
        up_slope[span, :] = jnp.where(up_open, gated, 0.0)
        slope = lift * (sigma + swish_alpha * gated * (1.0 - sigma))
        gate_slope[span, :] = jnp.where(gate_lin < clamp_limit, slope, 0.0)

    def compute(s, ready):
        rows = block(s)
        if not ready:
            remote(spot(s, near), spot(s, near), n_s.at[s], n_r.at[s], me, near).wait_recv()
            remote(spot(s, cross), spot(s, cross), m_s.at[s], m_r.at[s], me, near).wait_recv()
        d_act = dots(cot_rows[rows, :], down_ref[...], 1, 1)
        d_gate = (d_act * gate_slope[rows, :]).astype(bf16)
        d_up = (d_act * up_slope[rows, :]).astype(bf16)
        delta[rows, pl.ds(0, hidden)] = d_gate
        delta[rows, pl.ds(hidden, hidden)] = d_up
        cut = min(model, 1024)
        for j in range(model // cut):
            span = pl.ds(j * cut, cut)
            part[rows, span] = dots(delta[rows, :], pair_w[span, :], 1, 1).astype(bf16)
        part_near(s, 1).start()
        part_near(s, 0).start()

    def pair_up(s):
        rows = block(s)
        part_near(s, 1).wait_recv()
        pair = part[rows, lanes(far, width)].astype(f32) + pair_buf[1, rows].astype(f32)
        far_out[rows, :] = pair.astype(bf16)
        part_far(s).start()

    def finish(s, own):
        rows = block(s)
        part_near(s, 0).wait_recv()
        part_far(s).wait_recv()
        total = part[rows, lanes(t, width)].astype(f32)
        total = total + pair_buf[0, rows].astype(f32) + far_in[rows, :].astype(f32)
        if own:
            home[rows, :] = total.astype(bf16)
        else:
            done[rows, :] = total.astype(bf16)
            to_home(s).start()

    for s in across + [partner]:
        swap(s).start()
    fan(me)
    loads[3].wait()
    conv = conv_ref[...].astype(f32)
    sums = jnp.where(lane == 0, jnp.sum(conv, axis=1, keepdims=True), 0.0)
    sums = jnp.where(lane == 1, jnp.sum(conv * conv, axis=1, keepdims=True), sums)
    stat_ref[...] = jnp.transpose(sums)[:8]
    small = []
    for k, p in enumerate((near, far, cross)):
        c = remote(stat_ref, stats_ref.at[t], t_s.at[k], t_r.at[k], me, p)
        c.start()
        small.append(c)
    stats_ref[t] = stat_ref[...]
    for c in loads[4:9]:
        c.wait()
    pieces = 4
    slopes(0, pieces)
    arrive(partner)
    fan(partner)
    relay(me)
    fill = [functools.partial(slopes, p, pieces) for p in range(1, pieces)]
    count = len(arriving)

    def at(k):
        return arriving[k]

    def normalize():
        for c in small:
            c.wait_recv()
        total = functools.reduce(jnp.add, [stats_ref[k] for k in range(narrow)])
        total = jnp.transpose(total)
        mean = total[:, 0:1] / channels
        var = total[:, 1:2] / channels - mean * mean
        inverse = lax.rsqrt(var + norm_epsilon)
        hat = (conv_ref[...].astype(f32) - mean) * inverse
        normed = hat * gain_ref[...]
        sigma = jax.nn.sigmoid(normed)
        dev_ref[...] = inverse
        hat_ref[...] = hat
        conv_act[...] = (normed * sigma).astype(bf16)
        slope_ref[...] = sigma * (1.0 + normed * (1.0 - sigma)) * gain_ref[...]

    outs = [r["gate_stage"], r["up_stage"], r["down_stage"], own_sum, r["value_stage"], r["grad_stage"]]
    stores = [pltpu.make_async_copy(d, r["result"][k], o_s.at[k]) for k, d in enumerate(outs)]
    for i in range(count + 5):
        if i - 5 >= 0 and i - 5 < count:
            finish(at(i - 5), False)
        if 0 <= i - 3 < count:
            pair_up(at(i - 3))
        if 0 <= i - 2 < count:
            compute(at(i - 2), False)
        if i < count:
            arrive(at(i))
            fan(at(i))
        if i == 0:
            relay(partner)
        elif i - 1 < count:
            relay(at(i - 1))
        for _ in range(2 - i):
            fill.pop(0)()
        if i == min(3, count):
            normalize()
        if i == count:
            compute(partner, False)
            compute(me, False)
        if i == count + 2:
            pair_up(partner)
            pair_up(me)
            outs[2][...] = dots(act_ref[...], cot_rows[...], 0, 0).astype(bf16)
            stores[2].start()
        if i == count + 3:
            outs[0][...] = dots(in_ref[...], delta[:, :hidden], 0, 0).astype(bf16)
            stores[0].start()
        if i == count + 4:
            outs[1][...] = dots(in_ref[...], delta[:, hidden:], 0, 0).astype(bf16)
            stores[1].start()
    finish(partner, False)
    finish(me, True)
    for s in sp_peers:
        from_home(s).wait_recv()
    summed = dots(pick_any, home[...], 0, 0)
    mix_full[:, lanes(t, width)] = (cot_ref[...].astype(f32) + summed).astype(bf16)

    pieces = 2
    piece_rows = tokens // pieces

    def wide(k, column):
        return mix_full.at[pl.ds(k * piece_rows, piece_rows), lanes(column, width)]

    def wide_far(k):
        return remote(wide(k, t), wide(k, t), wf_s.at[k], wf_r.at[k], me, far)

    def wide_near(k):
        return remote(wide(k, t), wide(k, t), wn_s.at[k], wn_r.at[k], me, near)

    def wide_on(k):
        return remote(wide(k, far), wide(k, far), wm_s.at[k], wm_r.at[k], me, near)

    pairs = group // 2
    parity = lax.rem(me, 2)
    half = me // 2
    ahead, behind = lax.rem(me + 1, group), lax.rem(me + group - 1, group)
    alike = [lax.rem(half + o, pairs) for o in spread(pairs)]
    order = alike + [half]
    columns = [t, near, far, cross]
    sub = parts.shape[1]

    def pair_swap(q, c):
        side = lanes(columns[c], width)
        return remote(
            parts.at[2 * q + 1 - parity, :, side],
            pair_in.at[q, :, side],
            x_s.at[q, c],
            x_r.at[q, c],
            partner,
            t,
        )

    def slot_of(source, target):
        return lax.rem(target - source + pairs, pairs) - 1

    def passing(source, target, c):
        return others.at[slot_of(source, target), :, lanes(columns[c], width)], z_r.at[source, c]

    def scatter(q, c):
        slot, arrival = passing(half, q, c)
        source = pair_sum.at[q, :, lanes(columns[c], width)]
        return remote(source, slot, z_s.at[q, c], arrival, 2 * q + parity, t)

    def project(c):
        side = lanes(columns[c], width)
        product = dots(conv_act[...], mix_full[:, side], 0, 0)
        parts[:, :, side] = product.reshape(group, sub, width).astype(bf16)
        for q in order:
            pair_swap(q, c).start()

    def absorb(q, c, own):
        side = lanes(columns[c], width)
        pair_swap(q, c).wait_recv()
        both = parts[2 * q + parity, :, side].astype(f32) + pair_in[q, :, side].astype(f32)
        if own:
            own_sum[:, side] = both
        else:
            pair_sum[q, :, side] = both.astype(bf16)
            scatter(q, c).start()

    tasks = [functools.partial(absorb, q, c, k == pairs - 1) for c in range(narrow) for k, q in enumerate(order)]

    def run(number):
        for _ in range(min(number, len(tasks))):
            tasks.pop(0)()

    for k in range(pieces):
        wide_far(k).start()
    for k in range(pieces):
        wide_near(k).start()
    project(0)
    for k in range(pieces):
        wide_near(k).wait_recv()
    project(1)
    for k in range(pieces):
        wide_far(k).wait_recv()
        wide_on(k).start()
    run(pairs // 2)
    loads[9].wait()
    project(2)
    run(pairs // 2)
    for k in range(pieces):
        wide_on(k).wait_recv()
    ng = dots(mix_full[...], w_ref[...], 1, 1) * slope_ref[...]
    hat = hat_ref[...]
    sums = jnp.where(lane == 0, jnp.sum(ng, axis=1, keepdims=True), 0.0)
    sums = jnp.where(lane == 1, jnp.sum(ng * hat, axis=1, keepdims=True), sums)
    term_ref[...] = jnp.transpose(sums)[:8]
    terms = []
    for k, p in enumerate((near, far, cross)):
        terms.append(remote(term_ref, terms_ref.at[k], u_s.at[k], u_r.at[k], me, p))
        terms[k].start()
    run(pairs // 2)
    total = term_ref[...]
    for k, c in enumerate(terms):
        c.wait_recv()
        total = total + terms_ref[k]
    total = jnp.transpose(total)
    first, second = total[:, 0:1] / channels, total[:, 1:2] / channels
    extended[pl.ds(0, tokens), :] = dev_ref[...] * (ng - first - hat * second)
    halo = beyond.shape[0]
    halo_send = remote(extended.at[pl.ds(0, halo)], beyond, e_s.at[0], e_r.at[0], behind, t)
    halo_send.start()
    project(3)
    for c in loads[10:]:
        c.wait()

    reach = taps_ref.shape[0]
    step = 32
    strips = width // 128

    def convolve(index, carry):
        start = pl.multiple_of((index // strips) * step, step)
        column = lanes(lax.rem(index, strips), 128)
        total = jnp.zeros((step, 128), f32)
        window = extended[pl.ds(start, step + halo), column]
        for turn in range(8):
            shifted = window if turn == 0 else pltpu.roll(window, step + halo - turn, 0)
            for j in range(turn, reach, 8):
                total = total + taps_ref[reach - 1 - j : reach - j, column] * shifted[j - turn : j - turn + step]
        here = pl.ds(start, step)
        gate_sig = jax.nn.sigmoid(r["gate"][here, column].astype(f32))
        moved = total * gate_sig
        outs[4][here, column] = moved.astype(bf16)
        outs[5][here, column] = (moved * r["value"][here, column].astype(f32) * (1.0 - gate_sig)).astype(bf16)
        return carry

    turns = (tokens // step - 1) * strips
    rest = len(tasks) - 2
    marks = [turns * i // rest for i in range(rest + 1)]
    for i in range(rest):
        run(1)
        lax.fori_loop(marks[i], marks[i + 1], convolve, 0)
    run(1)
    halo_send.wait_recv()
    tail_rows = beyond[...]
    extended[pl.ds(tokens, halo), :] = jnp.where(me == group - 1, jnp.zeros_like(tail_rows), tail_rows)
    lax.fori_loop(turns, turns + strips, convolve, 0)
    stores[4].start()
    stores[5].start()
    run(1)
    for c in range(narrow):
        side = lanes(columns[c], width)
        total = own_sum[:, side]
        for q in alike:
            slot, arrival = passing(q, half, c)
            remote(pair_sum.at[q, :, side], slot, z_s.at[q, c], arrival, 2 * q + parity, t).wait_recv()
            total = total + others[slot_of(q, half), :, side].astype(f32)
        own_sum[:, side] = total
    stores[3].start()
    for s in [me] + sp_peers:
        to_far(s).wait_send()
        to_near(s).wait_send()
        onward(s).wait_send()
        part_near(s, 0).wait_send()
        part_near(s, 1).wait_send()
        part_far(s).wait_send()
    for s in sp_peers:
        swap(s).wait_send()
        to_home(s).wait_send()
    for c in small + terms:
        c.wait_send()
    for k in range(pieces):
        wide_far(k).wait_send()
        wide_near(k).wait_send()
        wide_on(k).wait_send()
    halo_send.wait_send()
    for c in range(narrow):
        for q in order:
            pair_swap(q, c).wait_send()
        for q in alike:
            scatter(q, c).wait_send()
    for c in stores:
        c.wait()


def whole_pass(*args):
    group, narrow = lax.axis_size("sp"), lax.axis_size("tp")
    ids, weight, cot, conv, gain, rows_in, gate_w, up_w, down_w, proj_w, taps, value, gate = args
    tokens, width = cot.shape
    slots, model = rows_in.shape
    hidden = down_w.shape[0]
    cap = slots // group
    pairs = group // 2
    sub = width // group
    halo = -(-(taps.shape[0] - 1) // 8) * 8
    f32, bf16 = jnp.float32, jnp.bfloat16
    dma = pltpu.SemaphoreType.DMA
    rows = (slots, width)
    tile = (tokens, width)
    results = [
        ((model, hidden), bf16),
        ((model, hidden), bf16),
        ((hidden, model), bf16),
        ((sub, model), f32),
        (tile, bf16),
        (tile, bf16),
    ]
    scratch = dict(
        ids=VMEM(ids.shape, ids.dtype),
        weight=VMEM(weight.shape, weight.dtype),
        cot=VMEM(tile, bf16),
        conv=VMEM(tile, bf16),
        gain=VMEM(gain.shape, f32),
        pair_w=VMEM((model, 2 * hidden), bf16),
        down=VMEM(down_w.shape, bf16),
        proj=VMEM(proj_w.shape, bf16),
        taps=VMEM(taps.shape, f32),
        value=VMEM(tile, bf16),
        gate=VMEM(tile, bf16),
        out=VMEM(rows, bf16),
        cot_rows=VMEM((slots, model), bf16),
        act=VMEM((slots, hidden), bf16),
        up_slope=VMEM((slots, hidden), f32),
        gate_slope=VMEM((slots, hidden), f32),
        delta=VMEM((slots, 2 * hidden), bf16),
        part=VMEM((slots, model), bf16),
        pair_buf=VMEM((2,) + rows, bf16),
        far_out=VMEM(rows, bf16),
        far_in=VMEM(rows, bf16),
        done=VMEM(rows, bf16),
        home=VMEM(rows, bf16),
        stat=VMEM((8, tokens), f32),
        stats=VMEM((narrow, 8, tokens), f32),
        term=VMEM((8, tokens), f32),
        terms=VMEM((narrow - 1, 8, tokens), f32),
        mix_full=VMEM((tokens, model), bf16),
        parts=VMEM((group, sub, model), bf16),
        pair_in=VMEM((pairs, sub, model), bf16),
        pair_sum=VMEM((pairs, sub, model), bf16),
        others=VMEM((pairs - 1, sub, model), bf16),
        own_sum=VMEM((sub, model), f32),
        extended=VMEM((tokens + halo, width), f32),
        beyond=VMEM((halo, width), f32),
        conv_act=VMEM(tile, bf16),
        hat=VMEM(tile, f32),
        slope=VMEM(tile, f32),
        dev=VMEM((tokens, 1), f32),
        gate_stage=VMEM((model, hidden), bf16),
        up_stage=VMEM((model, hidden), bf16),
        down_stage=VMEM((hidden, model), bf16),
        value_stage=VMEM(tile, bf16),
        grad_stage=VMEM(tile, bf16),
        l_s=dma((len(args),)),
        o_s=dma((len(results),)),
        e_s=dma((1,)),
        e_r=dma((1,)),
    )
    scratch["in"] = VMEM(rows_in.shape, bf16)
    for n in ("a", "n", "f", "m", "pf", "h"):
        scratch[n + "_s"] = scratch[n + "_r"] = dma((group,))
    scratch["pn_s"] = scratch["pn_r"] = dma((group, 2))
    for n in ("t", "u"):
        scratch[n + "_s"] = scratch[n + "_r"] = dma((narrow - 1,))
    for n in ("wn", "wf", "wm"):
        scratch[n + "_s"] = scratch[n + "_r"] = dma((2,))
    for n in ("x", "z"):
        scratch[n + "_s"] = scratch[n + "_r"] = dma((pairs, narrow))

    def body(*refs):
        whole_kernel(group, narrow, cap, len(args), len(results), tuple(scratch), *refs)

    return pl.pallas_call(
        body,
        name="whole_kernel",
        out_shape=tuple(jax.ShapeDtypeStruct(*x) for x in results),
        in_specs=[pl.BlockSpec(memory_space=pl.ANY)] * len(args),
        out_specs=[pl.BlockSpec(memory_space=pl.ANY)] * len(results),
        scratch_shapes=list(scratch.values()),
        compiler_params=pltpu.CompilerParams(
            collective_id=0, has_side_effects=True, vmem_limit_bytes=60 * 1024 * 1024
        ),
    )(*args)


def per_device(
    cot_out,
    route_ids,
    route_weight,
    expert_inputs,
    w_gate,
    w_up,
    w_down,
    w_proj,
    conv_out,
    channel_norm_gain,
    taps,
    value_pre,
    gate_pre,
):
    group_size = lax.axis_size("sp")
    rows_in = expert_inputs[0]
    slot_rows, model_width = rows_in.shape
    capacity = slot_rows // group_size
    fitted = -(-capacity // 16) * 16
    if fitted != capacity:
        rows_in = rows_in.reshape(group_size, capacity, model_width)
        rows_in = jnp.pad(rows_in, ((0, 0), (0, fitted - capacity), (0, 0)))
        rows_in = rows_in.reshape(group_size * fitted, model_width)
    grad_gate_part, grad_up_part, grad_down, grad_proj, grad_value, grad_gate = whole_pass(
        route_ids.T,
        route_weight.T,
        cot_out,
        conv_out,
        channel_norm_gain[None, :],
        rows_in,
        w_gate[0],
        w_up[0],
        w_down[0],
        w_proj,
        taps,
        value_pre,
        gate_pre,
    )
    return (
        grad_gate_part[None],
        grad_up_part[None],
        grad_down[None],
        grad_proj,
        grad_value,
        grad_gate,
    )


def solution(mesh):
    return jax.shard_map(
        per_device,
        mesh=mesh,
        in_specs=(
            P("sp", "tp"),
            P("sp", None),
            P("sp", None),
            P("sp", None, None),
            P("sp", None, "tp"),
            P("sp", None, "tp"),
            P("sp", "tp", None),
            P("tp", None),
            P("sp", "tp"),
            P("tp"),
            P(None, "tp"),
            P("sp", "tp"),
            P("sp", "tp"),
        ),
        out_specs=(
            P("sp", None, "tp"),
            P("sp", None, "tp"),
            P("sp", "tp", None),
            P(("tp", "sp"), None),
            P("sp", "tp"),
            P("sp", "tp"),
        ),
        check_vma=False,
    )
```

```python
import functools

import jax
import jax.numpy as jnp
from jax import lax
from jax.experimental import pallas as pl
from jax.experimental.pallas import tpu as pltpu
from jax.sharding import PartitionSpec as P

clamp_limit = 7.0
swish_alpha = 1.702
norm_epsilon = 1e-05
MESH = pl.DeviceIdType.MESH
VMEM = pltpu.VMEM


def lanes(index, width):
    return pl.ds(pl.multiple_of(index * width, width), width)


def places(group, narrow):
    me, t = lax.axis_index("sp"), lax.axis_index("tp")
    near = t + 1 - 2 * lax.rem(t, 2)
    far = lax.rem(t + narrow // 2, narrow)
    return me, t, near, far, lax.rem(near + narrow // 2, narrow)


def spread(pairs):
    return sorted(range(1, pairs), key=lambda o: abs(2 * o - pairs))


def nearest(here, count):
    def reaches(a, b):
        return (a - b + count) // count

    upper = reaches(here, count - 1 - here)
    inner = here + (count - 1 - 2 * here) * upper
    found = []
    for k in range(count - 1):
        lone = reaches(k, 2 * inner)
        both = k // 2 + 1 if k % 2 == 0 else -(k // 2 + 1)
        found.append(here + (1 - lone) * both + lone * (1 - 2 * upper) * (k - inner + 1))
    return found


def around(me, group):
    half, parity = me // 2, lax.rem(me, 2)
    across = [2 * z + side for z in nearest(half, group // 2) for side in (parity, 1 - parity)]
    return 2 * half + 1 - parity, across


def remote(src, dst, send, recv, sp, tp):
    return pltpu.make_async_remote_copy(
        src_ref=src, dst_ref=dst, send_sem=send, recv_sem=recv, device_id=(sp, tp), device_id_type=MESH
    )


def meet(peers):
    barrier = pltpu.get_barrier_semaphore()
    for sp, tp in peers:
        pl.semaphore_signal(barrier, inc=1, device_id=(sp, tp), device_id_type=MESH)
    pl.semaphore_wait(barrier, len(peers))


def dots(lhs, rhs, left, right):
    return lax.dot_general(lhs, rhs, (((left,), (right,)), ((), ())), preferred_element_type=jnp.float32)


small_loads = ("ids", "weight", "cot", "conv", "gain")


def whole_kernel(group, narrow, cap, inputs, results, names, *refs):
    r = dict(zip(names, refs[inputs + results :]))
    r["result"] = refs[inputs : inputs + results]
    ids_ref, weight_ref, cot_ref, conv_ref, gain_ref = (r[n] for n in small_loads)
    in_ref, pair_w, down_ref, w_ref, taps_ref = r["in"], r["pair_w"], r["down"], r["proj"], r["taps"]
    out_ref, cot_rows, act_ref, delta, part = r["out"], r["cot_rows"], r["act"], r["delta"], r["part"]
    up_slope, gate_slope, pair_buf = r["up_slope"], r["gate_slope"], r["pair_buf"]
    far_out, far_in, done, home = r["far_out"], r["far_in"], r["done"], r["home"]
    stat_ref, stats_ref, term_ref, terms_ref = r["stat"], r["stats"], r["term"], r["terms"]
    mix_full, parts, pair_in, pair_sum = r["mix_full"], r["parts"], r["pair_in"], r["pair_sum"]
    others, own_sum, extended, beyond = r["others"], r["own_sum"], r["extended"], r["beyond"]
    conv_act, hat_ref, slope_ref, dev_ref = r["conv_act"], r["hat"], r["slope"], r["dev"]
    a_s, a_r, n_s, n_r, f_s, f_r, m_s, m_r = (r[n] for n in ("a_s", "a_r", "n_s", "n_r", "f_s", "f_r", "m_s", "m_r"))
    pn_s, pn_r, pf_s, pf_r, h_s, h_r = (r[n] for n in ("pn_s", "pn_r", "pf_s", "pf_r", "h_s", "h_r"))
    t_s, t_r, u_s, u_r, l_s, o_s = (r[n] for n in ("t_s", "t_r", "u_s", "u_r", "l_s", "o_s"))
    wn_s, wn_r, wf_s, wf_r, wm_s, wm_r = (r[n] for n in ("wn_s", "wn_r", "wf_s", "wf_r", "wm_s", "wm_r"))
    x_s, x_r, z_s, z_r, e_s, e_r = (r[n] for n in ("x_s", "x_r", "z_s", "z_r", "e_s", "e_r"))
    f32, bf16 = jnp.float32, jnp.bfloat16
    me, t, near, far, cross = places(group, narrow)
    partner, across = around(me, group)
    arriving = across
    sp_peers = [partner] + across
    peers = [(p, t) for p in sp_peers] + [(me, near), (me, far), (me, cross)]
    barrier = pltpu.get_barrier_semaphore()
    for sp, tp in peers:
        pl.semaphore_signal(barrier, inc=1, device_id=(sp, tp), device_id_type=MESH)

    tokens, width = cot_ref.shape
    slots, model = cot_rows.shape
    hidden = down_ref.shape[0]
    chosen = ids_ref.shape[0]
    channels = width * narrow
    targets = [ids_ref, weight_ref, cot_ref, conv_ref, gain_ref, in_ref]
    targets += [pair_w.at[:, pl.ds(0, hidden)], pair_w.at[:, pl.ds(hidden, hidden)], down_ref]
    targets += [w_ref, taps_ref, r["value"], r["gate"]]
    loads = [pltpu.make_async_copy(refs[k], d, l_s.at[k]) for k, d in enumerate(targets)]
    for c in loads:
        c.start()
    for c in loads[:3]:
        c.wait()

    ids_rows = ids_ref[...]
    lane = lax.broadcasted_iota(jnp.int32, (tokens, 128), 1)
    row = lax.broadcasted_iota(jnp.int32, (8, tokens), 0)
    weight_rows = jnp.zeros((8, tokens), f32)
    for k in range(chosen):
        weight_rows = jnp.where(row == k, weight_ref[k : k + 1, :], weight_rows)
    weights = jnp.transpose(weight_rows)
    experts = -(-group // 8) * 8
    expert = lax.broadcasted_iota(jnp.int32, (experts, tokens), 0)
    hots = [ids_rows[k : k + 1] == expert for k in range(chosen)]
    hot = functools.reduce(jnp.logical_or, hots).astype(f32).astype(bf16)
    first = lax.broadcasted_iota(jnp.int32, (tokens, tokens), 0)
    second = lax.broadcasted_iota(jnp.int32, (tokens, tokens), 1)
    earlier = dots(hot, (first < second).astype(f32).astype(bf16), 1, 0)
    slot_row = lax.broadcasted_iota(jnp.int32, (slots, tokens), 0)
    picks = []
    outgoing = jnp.zeros((slots, width), f32)
    for k in range(chosen):
        slot = jnp.sum(jnp.where(hots[k], earlier, 0.0), axis=0, keepdims=True).astype(jnp.int32)
        dest = ids_rows[k : k + 1] * cap + slot
        pick = (slot_row == dest).astype(f32).astype(bf16)
        scaled = (weights[:, k : k + 1] * cot_ref[...].astype(f32)).astype(bf16)
        outgoing = outgoing + dots(pick, scaled, 1, 0)
        picks.append(pick)
    out_ref[...] = outgoing.astype(bf16)
    pick_any = functools.reduce(jnp.add, picks)

    def block(s):
        return pl.ds(pl.multiple_of(s * cap, cap), cap)

    def spot(s, column):
        return cot_rows.at[block(s), lanes(column, width)]

    cot_rows[block(me), lanes(t, width)] = out_ref[block(me), :]
    pl.semaphore_wait(barrier, len(peers))

    def swap(s):
        return remote(out_ref.at[block(s)], spot(me, t), a_s.at[s], a_r.at[me], s, t)

    def to_far(s):
        return remote(spot(s, t), spot(s, t), f_s.at[s], f_r.at[s], me, far)

    def to_near(s):
        return remote(spot(s, t), spot(s, t), n_s.at[s], n_r.at[s], me, near)

    def onward(s):
        return remote(spot(s, far), spot(s, far), m_s.at[s], m_r.at[s], me, near)

    def part_near(s, k):
        column = near if k == 0 else cross
        return remote(
            part.at[block(s), lanes(column, width)],
            pair_buf.at[k, block(s)],
            pn_s.at[s, k],
            pn_r.at[s, k],
            me,
            near,
        )

    def part_far(s):
        return remote(far_out.at[block(s)], far_in.at[block(s)], pf_s.at[s], pf_r.at[s], me, far)

    def to_home(s):
        return remote(done.at[block(s)], home.at[block(me)], h_s.at[s], h_r.at[me], s, t)

    def from_home(s):
        return remote(done.at[block(s)], home.at[block(s)], h_s.at[s], h_r.at[s], s, t)

    def arrive(s):
        remote(out_ref.at[block(s)], spot(s, t), a_s.at[s], a_r.at[s], s, t).wait_recv()

    def fan(s):
        to_far(s).start()
        to_near(s).start()

    def relay(s):
        to_far(s).wait_recv()
        onward(s).start()

    def slopes(piece, pieces):
        count = slots // pieces
        span = pl.ds(piece * count, count)
        both = jnp.dot(in_ref[span, :], pair_w[...], preferred_element_type=f32)
        gate_lin, up_lin = both[:, :hidden], both[:, hidden:]
        gate_c = jnp.minimum(gate_lin, clamp_limit)
        up_c = jnp.clip(up_lin, -clamp_limit, clamp_limit)
        sigma = jax.nn.sigmoid(swish_alpha * gate_c)
        lift, gated = up_c + 1.0, gate_c * sigma
        act_ref[span, :] = (lift * gated).astype(bf16)
        up_open = (up_lin > -clamp_limit) & (up_lin < clamp_limit)
        up_slope[span, :] = jnp.where(up_open, gated, 0.0)
        slope = lift * (sigma + swish_alpha * gated * (1.0 - sigma))
        gate_slope[span, :] = jnp.where(gate_lin < clamp_limit, slope, 0.0)

    def compute(s, ready):
        rows = block(s)
        if not ready:
            remote(spot(s, near), spot(s, near), n_s.at[s], n_r.at[s], me, near).wait_recv()
            remote(spot(s, cross), spot(s, cross), m_s.at[s], m_r.at[s], me, near).wait_recv()
        d_act = dots(cot_rows[rows, :], down_ref[...], 1, 1)
        d_gate = (d_act * gate_slope[rows, :]).astype(bf16)
        d_up = (d_act * up_slope[rows, :]).astype(bf16)
        delta[rows, pl.ds(0, hidden)] = d_gate
        delta[rows, pl.ds(hidden, hidden)] = d_up
        cut = min(model, 1024)
        for j in range(model // cut):
            span = pl.ds(j * cut, cut)
            part[rows, span] = dots(delta[rows, :], pair_w[span, :], 1, 1).astype(bf16)
        part_near(s, 1).start()
        part_near(s, 0).start()

    def pair_up(s):
        rows = block(s)
        part_near(s, 1).wait_recv()
        pair = part[rows, lanes(far, width)].astype(f32) + pair_buf[1, rows].astype(f32)
        far_out[rows, :] = pair.astype(bf16)
        part_far(s).start()

    def finish(s, own):
        rows = block(s)
        part_near(s, 0).wait_recv()
        part_far(s).wait_recv()
        total = part[rows, lanes(t, width)].astype(f32)
        total = total + pair_buf[0, rows].astype(f32) + far_in[rows, :].astype(f32)
        if own:
            home[rows, :] = total.astype(bf16)
        else:
            done[rows, :] = total.astype(bf16)
            to_home(s).start()

    for s in across + [partner]:
        swap(s).start()
    fan(me)
    loads[3].wait()
    conv = conv_ref[...].astype(f32)
    sums = jnp.where(lane == 0, jnp.sum(conv, axis=1, keepdims=True), 0.0)
    sums = jnp.where(lane == 1, jnp.sum(conv * conv, axis=1, keepdims=True), sums)
    stat_ref[...] = jnp.transpose(sums)[:8]
    small = []
    for k, p in enumerate((near, far, cross)):
        c = remote(stat_ref, stats_ref.at[t], t_s.at[k], t_r.at[k], me, p)
        c.start()
        small.append(c)
    stats_ref[t] = stat_ref[...]
    for c in loads[4:9]:
        c.wait()
    pieces = 4
    slopes(0, pieces)
    arrive(partner)
    fan(partner)
    relay(me)
    fill = [functools.partial(slopes, p, pieces) for p in range(1, pieces)]
    count = len(arriving)

    def at(k):
        return arriving[k]

    def normalize():
        for c in small:
            c.wait_recv()
        total = functools.reduce(jnp.add, [stats_ref[k] for k in range(narrow)])
        total = jnp.transpose(total)
        mean = total[:, 0:1] / channels
        var = total[:, 1:2] / channels - mean * mean
        inverse = lax.rsqrt(var + norm_epsilon)
        hat = (conv_ref[...].astype(f32) - mean) * inverse
        normed = hat * gain_ref[...]
        sigma = jax.nn.sigmoid(normed)
        dev_ref[...] = inverse
        hat_ref[...] = hat
        conv_act[...] = (normed * sigma).astype(bf16)
        slope_ref[...] = sigma * (1.0 + normed * (1.0 - sigma)) * gain_ref[...]

    outs = [r["gate_stage"], r["up_stage"], r["down_stage"], own_sum, r["value_stage"], r["grad_stage"]]
    stores = [pltpu.make_async_copy(d, r["result"][k], o_s.at[k]) for k, d in enumerate(outs)]
    for i in range(count + 5):
        if i - 5 >= 0 and i - 5 < count:
            finish(at(i - 5), False)
        if 0 <= i - 3 < count:
            pair_up(at(i - 3))
        if 0 <= i - 2 < count:
            compute(at(i - 2), False)
        if i < count:
            arrive(at(i))
            fan(at(i))
        if i == 0:
            relay(partner)
        elif i - 1 < count:
            relay(at(i - 1))
        for _ in range(2 - i):
            fill.pop(0)()
        if i == min(3, count):
            normalize()
        if i == count:
            compute(partner, False)
            compute(me, False)
        if i == count + 2:
            pair_up(partner)
            pair_up(me)
            outs[2][...] = dots(act_ref[...], cot_rows[...], 0, 0).astype(bf16)
            stores[2].start()
        if i == count + 3:
            outs[0][...] = dots(in_ref[...], delta[:, :hidden], 0, 0).astype(bf16)
            stores[0].start()
        if i == count + 4:
            outs[1][...] = dots(in_ref[...], delta[:, hidden:], 0, 0).astype(bf16)
            stores[1].start()
    finish(partner, False)
    finish(me, True)
    for s in sp_peers:
        from_home(s).wait_recv()
    summed = dots(pick_any, home[...], 0, 0)
    mix_full[:, lanes(t, width)] = (cot_ref[...].astype(f32) + summed).astype(bf16)

    pieces = 2
    piece_rows = tokens // pieces

    def wide(k, column):
        return mix_full.at[pl.ds(k * piece_rows, piece_rows), lanes(column, width)]

    def wide_far(k):
        return remote(wide(k, t), wide(k, t), wf_s.at[k], wf_r.at[k], me, far)

    def wide_near(k):
        return remote(wide(k, t), wide(k, t), wn_s.at[k], wn_r.at[k], me, near)

    def wide_on(k):
        return remote(wide(k, far), wide(k, far), wm_s.at[k], wm_r.at[k], me, near)

    pairs = group // 2
    parity = lax.rem(me, 2)
    half = me // 2
    ahead, behind = lax.rem(me + 1, group), lax.rem(me + group - 1, group)
    alike = [lax.rem(half + o, pairs) for o in spread(pairs)]
    order = alike + [half]
    columns = [t, near, far, cross]
    sub = parts.shape[1]

    def pair_swap(q, c):
        side = lanes(columns[c], width)
        return remote(
            parts.at[2 * q + 1 - parity, :, side],
            pair_in.at[q, :, side],
            x_s.at[q, c],
            x_r.at[q, c],
            partner,
            t,
        )

    def slot_of(source, target):
        return lax.rem(target - source + pairs, pairs) - 1

    def passing(source, target, c):
        return others.at[slot_of(source, target), :, lanes(columns[c], width)], z_r.at[source, c]

    def scatter(q, c):
        slot, arrival = passing(half, q, c)
        source = pair_sum.at[q, :, lanes(columns[c], width)]
        return remote(source, slot, z_s.at[q, c], arrival, 2 * q + parity, t)

    def project(c):
        side = lanes(columns[c], width)
        product = dots(conv_act[...], mix_full[:, side], 0, 0)
        parts[:, :, side] = product.reshape(group, sub, width).astype(bf16)
        for q in order:
            pair_swap(q, c).start()

    def absorb(q, c, own):
        side = lanes(columns[c], width)
        pair_swap(q, c).wait_recv()
        both = parts[2 * q + parity, :, side].astype(f32) + pair_in[q, :, side].astype(f32)
        if own:
            own_sum[:, side] = both
        else:
            pair_sum[q, :, side] = both.astype(bf16)
            scatter(q, c).start()

    tasks = [functools.partial(absorb, q, c, k == pairs - 1) for c in range(narrow) for k, q in enumerate(order)]

    def run(number):
        for _ in range(min(number, len(tasks))):
            tasks.pop(0)()

    for k in range(pieces):
        wide_far(k).start()
    for k in range(pieces):
        wide_near(k).start()
    project(0)
    for k in range(pieces):
        wide_near(k).wait_recv()
    project(1)
    for k in range(pieces):
        wide_far(k).wait_recv()
        wide_on(k).start()
    run(pairs // 2)
    loads[9].wait()
    project(2)
    run(pairs // 2)
    for k in range(pieces):
        wide_on(k).wait_recv()
    ng = dots(mix_full[...], w_ref[...], 1, 1) * slope_ref[...]
    hat = hat_ref[...]
    sums = jnp.where(lane == 0, jnp.sum(ng, axis=1, keepdims=True), 0.0)
    sums = jnp.where(lane == 1, jnp.sum(ng * hat, axis=1, keepdims=True), sums)
    term_ref[...] = jnp.transpose(sums)[:8]
    terms = []
    for k, p in enumerate((near, far, cross)):
        terms.append(remote(term_ref, terms_ref.at[k], u_s.at[k], u_r.at[k], me, p))
        terms[k].start()
    run(pairs // 2)
    total = term_ref[...]
    for k, c in enumerate(terms):
        c.wait_recv()
        total = total + terms_ref[k]
    total = jnp.transpose(total)
    first, second = total[:, 0:1] / channels, total[:, 1:2] / channels
    extended[pl.ds(0, tokens), :] = dev_ref[...] * (ng - first - hat * second)
    halo = beyond.shape[0]
    halo_send = remote(extended.at[pl.ds(0, halo)], beyond, e_s.at[0], e_r.at[0], behind, t)
    halo_send.start()
    project(3)
    for c in loads[10:]:
        c.wait()

    reach = taps_ref.shape[0]
    step = 32
    strips = width // 128

    def convolve(index, carry):
        start = pl.multiple_of((index // strips) * step, step)
        column = lanes(lax.rem(index, strips), 128)
        total = jnp.zeros((step, 128), f32)
        window = extended[pl.ds(start, step + halo), column]
        for turn in range(8):
            shifted = window if turn == 0 else pltpu.roll(window, step + halo - turn, 0)
            for j in range(turn, reach, 8):
                total = total + taps_ref[reach - 1 - j : reach - j, column] * shifted[j - turn : j - turn + step]
        here = pl.ds(start, step)
        gate_sig = jax.nn.sigmoid(r["gate"][here, column].astype(f32))
        moved = total * gate_sig
        outs[4][here, column] = moved.astype(bf16)
        outs[5][here, column] = (moved * r["value"][here, column].astype(f32) * (1.0 - gate_sig)).astype(bf16)
        return carry

    turns = (tokens // step - 1) * strips
    rest = len(tasks) - 2
    marks = [turns * i // rest for i in range(rest + 1)]
    for i in range(rest):
        run(1)
        lax.fori_loop(marks[i], marks[i + 1], convolve, 0)
    run(1)
    halo_send.wait_recv()
    tail_rows = beyond[...]
    extended[pl.ds(tokens, halo), :] = jnp.where(me == group - 1, jnp.zeros_like(tail_rows), tail_rows)
    lax.fori_loop(turns, turns + strips, convolve, 0)
    stores[4].start()
    stores[5].start()
    run(1)
    for c in range(narrow):
        side = lanes(columns[c], width)
        total = own_sum[:, side]
        for q in alike:
            slot, arrival = passing(q, half, c)
            remote(pair_sum.at[q, :, side], slot, z_s.at[q, c], arrival, 2 * q + parity, t).wait_recv()
            total = total + others[slot_of(q, half), :, side].astype(f32)
        own_sum[:, side] = total
    stores[3].start()
    for s in [me] + sp_peers:
        to_far(s).wait_send()
        to_near(s).wait_send()
        onward(s).wait_send()
        part_near(s, 0).wait_send()
        part_near(s, 1).wait_send()
        part_far(s).wait_send()
    for s in sp_peers:
        swap(s).wait_send()
        to_home(s).wait_send()
    for c in small + terms:
        c.wait_send()
    for k in range(pieces):
        wide_far(k).wait_send()
        wide_near(k).wait_send()
        wide_on(k).wait_send()
    halo_send.wait_send()
    for c in range(narrow):
        for q in order:
            pair_swap(q, c).wait_send()
        for q in alike:
            scatter(q, c).wait_send()
    for c in stores:
        c.wait()


def whole_pass(*args):
    group, narrow = lax.axis_size("sp"), lax.axis_size("tp")
    ids, weight, cot, conv, gain, rows_in, gate_w, up_w, down_w, proj_w, taps, value, gate = args
    tokens, width = cot.shape
    slots, model = rows_in.shape
    hidden = down_w.shape[0]
    cap = slots // group
    pairs = group // 2
    sub = width // group
    halo = -(-(taps.shape[0] - 1) // 8) * 8
    f32, bf16 = jnp.float32, jnp.bfloat16
    dma = pltpu.SemaphoreType.DMA
    rows = (slots, width)
    tile = (tokens, width)
    results = [
        ((model, hidden), bf16),
        ((model, hidden), bf16),
        ((hidden, model), bf16),
        ((sub, model), f32),
        (tile, bf16),
        (tile, bf16),
    ]
    scratch = dict(
        ids=VMEM(ids.shape, ids.dtype),
        weight=VMEM(weight.shape, weight.dtype),
        cot=VMEM(tile, bf16),
        conv=VMEM(tile, bf16),
        gain=VMEM(gain.shape, f32),
        pair_w=VMEM((model, 2 * hidden), bf16),
        down=VMEM(down_w.shape, bf16),
        proj=VMEM(proj_w.shape, bf16),
        taps=VMEM(taps.shape, f32),
        value=VMEM(tile, bf16),
        gate=VMEM(tile, bf16),
        out=VMEM(rows, bf16),
        cot_rows=VMEM((slots, model), bf16),
        act=VMEM((slots, hidden), bf16),
        up_slope=VMEM((slots, hidden), f32),
        gate_slope=VMEM((slots, hidden), f32),
        delta=VMEM((slots, 2 * hidden), bf16),
        part=VMEM((slots, model), bf16),
        pair_buf=VMEM((2,) + rows, bf16),
        far_out=VMEM(rows, bf16),
        far_in=VMEM(rows, bf16),
        done=VMEM(rows, bf16),
        home=VMEM(rows, bf16),
        stat=VMEM((8, tokens), f32),
        stats=VMEM((narrow, 8, tokens), f32),
        term=VMEM((8, tokens), f32),
        terms=VMEM((narrow - 1, 8, tokens), f32),
        mix_full=VMEM((tokens, model), bf16),
        parts=VMEM((group, sub, model), bf16),
        pair_in=VMEM((pairs, sub, model), bf16),
        pair_sum=VMEM((pairs, sub, model), bf16),
        others=VMEM((pairs - 1, sub, model), bf16),
        own_sum=VMEM((sub, model), f32),
        extended=VMEM((tokens + halo, width), f32),
        beyond=VMEM((halo, width), f32),
        conv_act=VMEM(tile, bf16),
        hat=VMEM(tile, f32),
        slope=VMEM(tile, f32),
        dev=VMEM((tokens, 1), f32),
        gate_stage=VMEM((model, hidden), bf16),
        up_stage=VMEM((model, hidden), bf16),
        down_stage=VMEM((hidden, model), bf16),
        value_stage=VMEM(tile, bf16),
        grad_stage=VMEM(tile, bf16),
        l_s=dma((len(args),)),
        o_s=dma((len(results),)),
        e_s=dma((1,)),
        e_r=dma((1,)),
    )
    scratch["in"] = VMEM(rows_in.shape, bf16)
    for n in ("a", "n", "f", "m", "pf", "h"):
        scratch[n + "_s"] = scratch[n + "_r"] = dma((group,))
    scratch["pn_s"] = scratch["pn_r"] = dma((group, 2))
    for n in ("t", "u"):
        scratch[n + "_s"] = scratch[n + "_r"] = dma((narrow - 1,))
    for n in ("wn", "wf", "wm"):
        scratch[n + "_s"] = scratch[n + "_r"] = dma((2,))
    for n in ("x", "z"):
        scratch[n + "_s"] = scratch[n + "_r"] = dma((pairs, narrow))

    def body(*refs):
        whole_kernel(group, narrow, cap, len(args), len(results), tuple(scratch), *refs)

    return pl.pallas_call(
        body,
        name="whole_kernel",
        out_shape=tuple(jax.ShapeDtypeStruct(*x) for x in results),
        in_specs=[pl.BlockSpec(memory_space=pltpu.HBM)] * len(args),
        out_specs=[pl.BlockSpec(memory_space=pl.ANY)] * len(results),
        scratch_shapes=list(scratch.values()),
        compiler_params=pltpu.CompilerParams(
            collective_id=0, has_side_effects=True, vmem_limit_bytes=48 * 1024 * 1024
        ),
    )(*[pltpu.with_memory_space_constraint(x, pltpu.HBM) for x in args])


def emit_kernel(count, *refs):
    sems = refs[-1]
    copies = [pltpu.make_async_copy(refs[k], refs[count + k], sems.at[k]) for k in range(count)]
    for c in copies:
        c.start()
    for c in copies:
        c.wait()


def emit(*results):
    return pl.pallas_call(
        functools.partial(emit_kernel, len(results)),
        name="emit",
        out_shape=tuple(jax.ShapeDtypeStruct(x.shape, x.dtype) for x in results),
        in_specs=[pl.BlockSpec(memory_space=pl.ANY)] * len(results),
        out_specs=[pl.BlockSpec(memory_space=pltpu.HBM)] * len(results),
        scratch_shapes=[pltpu.SemaphoreType.DMA((len(results),))],
        compiler_params=pltpu.CompilerParams(vmem_limit_bytes=1024 * 1024),
    )(*results)


def per_device(
    cot_out,
    route_ids,
    route_weight,
    expert_inputs,
    w_gate,
    w_up,
    w_down,
    w_proj,
    conv_out,
    channel_norm_gain,
    taps,
    value_pre,
    gate_pre,
):
    group_size = lax.axis_size("sp")
    rows_in = expert_inputs[0]
    slot_rows, model_width = rows_in.shape
    capacity = slot_rows // group_size
    fitted = -(-capacity // 16) * 16
    if fitted != capacity:
        rows_in = rows_in.reshape(group_size, capacity, model_width)
        rows_in = jnp.pad(rows_in, ((0, 0), (0, fitted - capacity), (0, 0)))
        rows_in = rows_in.reshape(group_size * fitted, model_width)
    grad_gate_part, grad_up_part, grad_down, grad_proj, grad_value, grad_gate = emit(
        *whole_pass(
        route_ids.T,
        route_weight.T,
        cot_out,
        conv_out,
        channel_norm_gain[None, :],
        rows_in,
        w_gate[0],
        w_up[0],
        w_down[0],
        w_proj,
        taps,
        value_pre,
        gate_pre,
        )
    )
    return (
        grad_gate_part[None],
        grad_up_part[None],
        grad_down[None],
        grad_proj,
        grad_value,
        grad_gate,
    )


def solution(mesh):
    return jax.shard_map(
        per_device,
        mesh=mesh,
        in_specs=(
            P("sp", "tp"),
            P("sp", None),
            P("sp", None),
            P("sp", None, None),
            P("sp", None, "tp"),
            P("sp", None, "tp"),
            P("sp", "tp", None),
            P("tp", None),
            P("sp", "tp"),
            P("tp"),
            P(None, "tp"),
            P("sp", "tp"),
            P("sp", "tp"),
        ),
        out_specs=(
            P("sp", None, "tp"),
            P("sp", None, "tp"),
            P("sp", "tp", None),
            P(("tp", "sp"), None),
            P("sp", "tp"),
            P("sp", "tp"),
        ),
        check_vma=False,
    )
```

```python
import functools

import jax
import jax.numpy as jnp
from jax import lax
from jax.experimental import pallas as pl
from jax.experimental.pallas import tpu as pltpu
from jax.sharding import PartitionSpec as P

clamp_limit = 7.0
swish_alpha = 1.702
norm_epsilon = 1e-05
MESH = pl.DeviceIdType.MESH
VMEM = pltpu.VMEM


def lanes(index, width):
    return pl.ds(pl.multiple_of(index * width, width), width)


def places(group, narrow):
    me, t = lax.axis_index("sp"), lax.axis_index("tp")
    near = t + 1 - 2 * lax.rem(t, 2)
    far = lax.rem(t + narrow // 2, narrow)
    return me, t, near, far, lax.rem(near + narrow // 2, narrow)


def spread(pairs):
    return sorted(range(1, pairs), key=lambda o: abs(2 * o - pairs))


def nearest(here, count):
    def reaches(a, b):
        return (a - b + count) // count

    upper = reaches(here, count - 1 - here)
    inner = here + (count - 1 - 2 * here) * upper
    found = []
    for k in range(count - 1):
        lone = reaches(k, 2 * inner)
        both = k // 2 + 1 if k % 2 == 0 else -(k // 2 + 1)
        found.append(here + (1 - lone) * both + lone * (1 - 2 * upper) * (k - inner + 1))
    return found


def around(me, group):
    half, parity = me // 2, lax.rem(me, 2)
    across = [2 * z + side for z in nearest(half, group // 2) for side in (parity, 1 - parity)]
    return 2 * half + 1 - parity, across


def remote(src, dst, send, recv, sp, tp):
    return pltpu.make_async_remote_copy(
        src_ref=src, dst_ref=dst, send_sem=send, recv_sem=recv, device_id=(sp, tp), device_id_type=MESH
    )


def meet(peers):
    barrier = pltpu.get_barrier_semaphore()
    for sp, tp in peers:
        pl.semaphore_signal(barrier, inc=1, device_id=(sp, tp), device_id_type=MESH)
    pl.semaphore_wait(barrier, len(peers))


def dots(lhs, rhs, left, right):
    return lax.dot_general(lhs, rhs, (((left,), (right,)), ((), ())), preferred_element_type=jnp.float32)


small_loads = ("ids", "weight", "cot", "conv", "gain")


def whole_kernel(group, narrow, cap, inputs, results, names, *refs):
    r = dict(zip(names, refs[inputs + results :]))
    r["result"] = refs[inputs : inputs + results]
    ids_ref, weight_ref, cot_ref, conv_ref, gain_ref = (r[n] for n in small_loads)
    in_ref, pair_w, down_ref, w_ref, taps_ref = r["in"], r["pair_w"], r["down"], r["proj"], r["taps"]
    out_ref, cot_rows, act_ref, delta, part = r["out"], r["cot_rows"], r["act"], r["delta"], r["part"]
    up_slope, gate_slope, pair_buf = r["up_slope"], r["gate_slope"], r["pair_buf"]
    far_out, far_in, done, home = r["far_out"], r["far_in"], r["done"], r["home"]
    stat_ref, stats_ref, term_ref, terms_ref = r["stat"], r["stats"], r["term"], r["terms"]
    mix_both, product, kept, own_sum = r["mix_both"], r["product"], r["kept"], r["own_sum"]
    extended, beyond = r["extended"], r["beyond"]
    conv_act, hat_ref, slope_ref, dev_ref = r["conv_act"], r["hat"], r["slope"], r["dev"]
    a_s, a_r, n_s, n_r, f_s, f_r, m_s, m_r = (r[n] for n in ("a_s", "a_r", "n_s", "n_r", "f_s", "f_r", "m_s", "m_r"))
    pn_s, pn_r, pf_s, pf_r, h_s, h_r = (r[n] for n in ("pn_s", "pn_r", "pf_s", "pf_r", "h_s", "h_r"))
    t_s, t_r, u_s, u_r, l_s, o_s = (r[n] for n in ("t_s", "t_r", "u_s", "u_r", "l_s", "o_s"))
    wn_s, wn_r, wf_s, wf_r, wm_s, wm_r = (r[n] for n in ("wn_s", "wn_r", "wf_s", "wf_r", "wm_s", "wm_r"))
    x_s, x_r, y_s, y_r, e_s, e_r = (r[n] for n in ("x_s", "x_r", "y_s", "y_r", "e_s", "e_r"))
    f32, bf16 = jnp.float32, jnp.bfloat16
    me, t, near, far, cross = places(group, narrow)
    partner, across = around(me, group)
    arriving = across
    sp_peers = [partner] + across
    peers = [(p, t) for p in sp_peers] + [(me, near), (me, far), (me, cross)]
    barrier = pltpu.get_barrier_semaphore()
    for sp, tp in peers:
        pl.semaphore_signal(barrier, inc=1, device_id=(sp, tp), device_id_type=MESH)

    tokens, width = cot_ref.shape
    slots, model = cot_rows.shape
    hidden = down_ref.shape[0]
    chosen = ids_ref.shape[0]
    channels = width * narrow
    targets = [ids_ref, weight_ref, cot_ref, conv_ref, gain_ref, in_ref]
    targets += [pair_w.at[:, pl.ds(0, hidden)], pair_w.at[:, pl.ds(hidden, hidden)], down_ref]
    targets += [w_ref, taps_ref, r["value"], r["gate"]]
    loads = [pltpu.make_async_copy(refs[k], d, l_s.at[k]) for k, d in enumerate(targets)]
    for c in loads:
        c.start()
    for c in loads[:3]:
        c.wait()

    ids_rows = ids_ref[...]
    lane = lax.broadcasted_iota(jnp.int32, (tokens, 128), 1)
    row = lax.broadcasted_iota(jnp.int32, (8, tokens), 0)
    weight_rows = jnp.zeros((8, tokens), f32)
    for k in range(chosen):
        weight_rows = jnp.where(row == k, weight_ref[k : k + 1, :], weight_rows)
    weights = jnp.transpose(weight_rows)
    experts = -(-group // 8) * 8
    expert = lax.broadcasted_iota(jnp.int32, (experts, tokens), 0)
    hots = [ids_rows[k : k + 1] == expert for k in range(chosen)]
    hot = functools.reduce(jnp.logical_or, hots).astype(f32).astype(bf16)
    first = lax.broadcasted_iota(jnp.int32, (tokens, tokens), 0)
    second = lax.broadcasted_iota(jnp.int32, (tokens, tokens), 1)
    earlier = dots(hot, (first < second).astype(f32).astype(bf16), 1, 0)
    slot_row = lax.broadcasted_iota(jnp.int32, (slots, tokens), 0)
    picks = []
    outgoing = jnp.zeros((slots, width), f32)
    for k in range(chosen):
        slot = jnp.sum(jnp.where(hots[k], earlier, 0.0), axis=0, keepdims=True).astype(jnp.int32)
        dest = ids_rows[k : k + 1] * cap + slot
        pick = (slot_row == dest).astype(f32).astype(bf16)
        scaled = (weights[:, k : k + 1] * cot_ref[...].astype(f32)).astype(bf16)
        outgoing = outgoing + dots(pick, scaled, 1, 0)
        picks.append(pick)
    out_ref[...] = outgoing.astype(bf16)
    pick_any = functools.reduce(jnp.add, picks)

    def block(s):
        return pl.ds(pl.multiple_of(s * cap, cap), cap)

    def spot(s, column):
        return cot_rows.at[block(s), lanes(column, width)]

    cot_rows[block(me), lanes(t, width)] = out_ref[block(me), :]
    pl.semaphore_wait(barrier, len(peers))

    def swap(s):
        return remote(out_ref.at[block(s)], spot(me, t), a_s.at[s], a_r.at[me], s, t)

    def to_far(s):
        return remote(spot(s, t), spot(s, t), f_s.at[s], f_r.at[s], me, far)

    def to_near(s):
        return remote(spot(s, t), spot(s, t), n_s.at[s], n_r.at[s], me, near)

    def onward(s):
        return remote(spot(s, far), spot(s, far), m_s.at[s], m_r.at[s], me, near)

    hw = width // 2

    def piece_of(column, h):
        return pl.ds(pl.multiple_of(column * width + h * hw, hw), hw)

    def part_near(s, k, h):
        column = near if k == 0 else cross
        return remote(
            part.at[block(s), piece_of(column, h)],
            pair_buf.at[k, block(s), pl.ds(h * hw, hw)],
            pn_s.at[s, 2 * k + h],
            pn_r.at[s, 2 * k + h],
            me,
            near,
        )

    def part_far(s, h):
        side = pl.ds(h * hw, hw)
        return remote(far_out.at[block(s), side], far_in.at[block(s), side], pf_s.at[s, h], pf_r.at[s, h], me, far)

    def to_home(s, h):
        side = pl.ds(h * hw, hw)
        return remote(done.at[block(s), side], home.at[block(me), side], h_s.at[s, h], h_r.at[me, h], s, t)

    def from_home(s, h):
        side = pl.ds(h * hw, hw)
        return remote(done.at[block(s), side], home.at[block(s), side], h_s.at[s, h], h_r.at[s, h], s, t)

    def arrive(s):
        remote(out_ref.at[block(s)], spot(s, t), a_s.at[s], a_r.at[s], s, t).wait_recv()

    def fan(s):
        to_far(s).start()
        to_near(s).start()

    def relay(s):
        to_far(s).wait_recv()
        onward(s).start()

    def slopes(piece, pieces):
        count = slots // pieces
        span = pl.ds(piece * count, count)
        both = jnp.dot(in_ref[span, :], pair_w[...], preferred_element_type=f32)
        gate_lin, up_lin = both[:, :hidden], both[:, hidden:]
        gate_c = jnp.minimum(gate_lin, clamp_limit)
        up_c = jnp.clip(up_lin, -clamp_limit, clamp_limit)
        sigma = jax.nn.sigmoid(swish_alpha * gate_c)
        lift, gated = up_c + 1.0, gate_c * sigma
        act_ref[span, :] = (lift * gated).astype(bf16)
        up_open = (up_lin > -clamp_limit) & (up_lin < clamp_limit)
        up_slope[span, :] = jnp.where(up_open, gated, 0.0)
        slope = lift * (sigma + swish_alpha * gated * (1.0 - sigma))
        gate_slope[span, :] = jnp.where(gate_lin < clamp_limit, slope, 0.0)

    def compute(s, ready):
        rows = block(s)
        if not ready:
            remote(spot(s, near), spot(s, near), n_s.at[s], n_r.at[s], me, near).wait_recv()
            remote(spot(s, cross), spot(s, cross), m_s.at[s], m_r.at[s], me, near).wait_recv()
        d_act = dots(cot_rows[rows, :], r["down_t"][...], 1, 0)
        d_gate = (d_act * gate_slope[rows, :]).astype(bf16)
        d_up = (d_act * up_slope[rows, :]).astype(bf16)
        delta[rows, pl.ds(0, hidden)] = d_gate
        delta[rows, pl.ds(hidden, hidden)] = d_up
        cut = min(model, 1024)
        for j in range(model // cut):
            span = pl.ds(j * cut, cut)
            part[rows, span] = dots(delta[rows, :], r["pair_t"][:, span], 1, 0).astype(bf16)
        for h in range(2):
            part_near(s, 1, h).start()
            part_near(s, 0, h).start()

    def pair_up(s, h):
        rows = block(s)
        side = pl.ds(h * hw, hw)
        part_near(s, 1, h).wait_recv()
        pair = part[rows, piece_of(far, h)].astype(f32) + pair_buf[1, rows, side].astype(f32)
        far_out[rows, side] = pair.astype(bf16)
        part_far(s, h).start()

    def finish(s, h, own):
        rows = block(s)
        side = pl.ds(h * hw, hw)
        part_near(s, 0, h).wait_recv()
        part_far(s, h).wait_recv()
        total = part[rows, piece_of(t, h)].astype(f32)
        total = total + pair_buf[0, rows, side].astype(f32) + far_in[rows, side].astype(f32)
        if own:
            home[rows, side] = total.astype(bf16)
        else:
            done[rows, side] = total.astype(bf16)
            to_home(s, h).start()

    for s in across + [partner]:
        swap(s).start()
    fan(me)
    loads[3].wait()
    conv = conv_ref[...].astype(f32)
    sums = jnp.where(lane == 0, jnp.sum(conv, axis=1, keepdims=True), 0.0)
    sums = jnp.where(lane == 1, jnp.sum(conv * conv, axis=1, keepdims=True), sums)
    stat_ref[...] = jnp.transpose(sums)[:8]
    small = []
    for k, p in enumerate((near, far, cross)):
        c = remote(stat_ref, stats_ref.at[t], t_s.at[k], t_r.at[k], me, p)
        c.start()
        small.append(c)
    stats_ref[t] = stat_ref[...]
    for c in loads[4:9]:
        c.wait()
    pieces = 4
    slopes(0, pieces)
    slopes(1, pieces)
    r["down_t"][...] = jnp.transpose(down_ref[...])
    r["pair_t"][...] = jnp.transpose(pair_w[...])
    arrive(partner)
    fan(partner)
    slopes(2, pieces)
    slopes(3, pieces)
    relay(me)
    count = len(arriving)

    def at(k):
        return arriving[k]

    act_send = remote(
        conv_act.at[pl.ds(0, tokens)], conv_act.at[pl.ds(tokens, tokens)], e_s.at[1], e_r.at[1], partner, t
    )

    def normalize():
        for c in small:
            c.wait_recv()
        total = functools.reduce(jnp.add, [stats_ref[k] for k in range(narrow)])
        total = jnp.transpose(total)
        mean = total[:, 0:1] / channels
        var = total[:, 1:2] / channels - mean * mean
        inverse = lax.rsqrt(var + norm_epsilon)
        hat = (conv_ref[...].astype(f32) - mean) * inverse
        normed = hat * gain_ref[...]
        sigma = jax.nn.sigmoid(normed)
        dev_ref[...] = inverse
        hat_ref[...] = hat
        conv_act[pl.ds(0, tokens), :] = (normed * sigma).astype(bf16)
        act_send.start()
        slope_ref[...] = sigma * (1.0 + normed * (1.0 - sigma)) * gain_ref[...]

    outs = [r["gate_stage"], r["up_stage"], r["down_stage"], own_sum, r["value_stage"], r["grad_stage"]]
    stores = [pltpu.make_async_copy(d, r["result"][k], o_s.at[k]) for k, d in enumerate(outs)]
    pairs = group // 2
    parity = lax.rem(me, 2)
    half = me // 2
    ahead, behind = lax.rem(me + 1, group), lax.rem(me + group - 1, group)
    columns = [t, near, far, cross]
    sub = product.shape[1]
    levels = pairs.bit_length() - 1
    bits = [lax.rem(half // 2**j, 2) for j in range(levels)]
    halo = beyond.shape[0]

    def mixed(b, column, h):
        return mix_both.at[pl.ds(b * tokens, tokens), piece_of(column, h)]

    def wide_x(h):
        return remote(mixed(0, t, h), mixed(1, t, h), x_s.at[h], x_r.at[h], partner, t)

    def wide_far(b, h):
        return remote(mixed(b, t, h), mixed(b, t, h), wf_s.at[b, h], wf_r.at[b, h], me, far)

    def wide_near(b, h):
        return remote(mixed(b, t, h), mixed(b, t, h), wn_s.at[b, h], wn_r.at[b, h], me, near)

    def wide_on(b, h):
        return remote(mixed(b, far, h), mixed(b, far, h), wm_s.at[b, h], wm_r.at[b, h], me, near)

    def begin(h):
        for s in sp_peers:
            from_home(s, h).wait_recv()
        side = pl.ds(h * hw, hw)
        summed = dots(pick_any, home[:, side], 0, 0)
        mix_both[pl.ds(0, tokens), piece_of(t, h)] = (cot_ref[:, side].astype(f32) + summed).astype(bf16)
        wide_x(h).start()
        wide_far(0, h).start()
        wide_near(0, h).start()

    def share(h):
        wide_x(h).wait_recv()
        wide_far(1, h).start()
        wide_near(1, h).start()

    def pass_on(b, h):
        wide_far(b, h).wait_recv()
        wide_on(b, h).start()

    def gathered(kind, b, h):
        if kind == 1:
            spot_of, send, recv = mixed(b, near, h), wn_s, wn_r
        else:
            spot_of, send, recv = mixed(b, cross, h), wm_s, wm_r
        remote(spot_of, spot_of, send.at[b, h], recv.at[b, h], me, near).wait_recv()

    def trade(g, j):
        peer = 2 * (half + (1 - 2 * bits[j]) * 2**j) + parity
        return remote(r["go%d" % j].at[g], r["come%d" % j].at[g], y_s.at[g, j], y_r.at[g, j], peer, t)

    def project(c, h):
        g = 2 * c + h
        value = dots(conv_act[...], mix_both[:, piece_of(columns[c], h)], 0, 0)
        product[...] = value.reshape(group, sub, hw)
        for k in range(pairs // 2):
            r["go0"][g, k] = product[2 * (2 * k + 1 - bits[0]) + parity].astype(bf16)
            kept[g, k] = product[2 * (2 * k + bits[0]) + parity]
        trade(g, 0).start()

    def fold(c, h, j):
        g = 2 * c + h
        trade(g, j - 1).wait_recv()
        left = pairs >> j
        for k in range(left):
            kept[g, k] = kept[g, k] + r["come%d" % (j - 1)][g, k].astype(f32)
        if j < levels:
            for k in range(left // 2):
                r["go%d" % j][g, k] = kept[g, 2 * k + 1 - bits[j]].astype(bf16)
            for k in range(left // 2):
                kept[g, k] = kept[g, 2 * k + bits[j]]
            trade(g, j).start()
        else:
            own_sum[:, piece_of(columns[c], h)] = kept[g, 0]

    later = [functools.partial(pair_up, s, 1) for s in [me, partner] + arriving]
    blocks = [me, partner] + arriving
    for i in range(2, group + 4):
        if i < group:
            arrive(blocks[i])
            fan(blocks[i])
        if i - 1 < group:
            relay(blocks[i - 1])
        if i == min(5, group):
            normalize()
        if i - 2 < group:
            compute(blocks[i - 2], False)
        if 0 <= i - 3 < group:
            pair_up(blocks[i - 3], 0)
        if 0 <= i - 5 < group:
            finish(blocks[i - 5], 0, i == 5)
        if i > group:
            for _ in range(len(later) // (group + 4 - i)):
                later.pop(0)()
    finish(blocks[group - 1], 0, False)
    ending = [functools.partial(finish, s, 1, s is me) for s in blocks]
    for f in ending[: group // 2]:
        f()
    outs[2][...] = dots(act_ref[...], cot_rows[...], 0, 0).astype(bf16)
    stores[2].start()
    begin(0)
    for f in ending[group // 2 :]:
        f()
    outs[0][...] = dots(in_ref[...], delta[:, :hidden], 0, 0).astype(bf16)
    stores[0].start()
    share(0)
    act_send.wait_recv()
    project(0, 0)
    pass_on(0, 0)
    gathered(1, 0, 0)
    gathered(1, 1, 0)
    project(1, 0)
    begin(1)
    pass_on(1, 0)
    project(2, 0)
    gathered(2, 0, 0)
    gathered(2, 1, 0)
    project(3, 0)
    outs[1][...] = dots(in_ref[...], delta[:, hidden:], 0, 0).astype(bf16)
    stores[1].start()
    fold(0, 0, 1)
    fold(1, 0, 1)
    share(1)
    project(0, 1)
    pass_on(0, 1)
    gathered(1, 0, 1)
    gathered(1, 1, 1)
    project(1, 1)
    fold(2, 0, 1)
    fold(3, 0, 1)
    loads[9].wait()
    gathered(2, 0, 1)
    ng = dots(mix_both[pl.ds(0, tokens), :], w_ref[...], 1, 1) * slope_ref[...]
    hat = hat_ref[...]
    sums = jnp.where(lane == 0, jnp.sum(ng, axis=1, keepdims=True), 0.0)
    sums = jnp.where(lane == 1, jnp.sum(ng * hat, axis=1, keepdims=True), sums)
    term_ref[...] = jnp.transpose(sums)[:8]
    terms = []
    for k, p in enumerate((near, far, cross)):
        terms.append(remote(term_ref, terms_ref.at[k], u_s.at[k], u_r.at[k], me, p))
        terms[k].start()
    pass_on(1, 1)
    project(2, 1)
    fold(0, 1, 1)
    gathered(2, 1, 1)
    project(3, 1)
    total = term_ref[...]
    for k, c in enumerate(terms):
        c.wait_recv()
        total = total + terms_ref[k]
    total = jnp.transpose(total)
    first, second = total[:, 0:1] / channels, total[:, 1:2] / channels
    extended[pl.ds(0, tokens), :] = dev_ref[...] * (ng - first - hat * second)
    halo_send = remote(extended.at[pl.ds(0, halo)], beyond, e_s.at[0], e_r.at[0], behind, t)
    halo_send.start()
    for c in loads[10:]:
        c.wait()

    reach = taps_ref.shape[0]
    step = 32
    strips = width // 128

    def convolve(index, carry):
        start = pl.multiple_of((index // strips) * step, step)
        column = lanes(lax.rem(index, strips), 128)
        total = jnp.zeros((step, 128), f32)
        window = extended[pl.ds(start, step + halo), column]
        for turn in range(8):
            shifted = window if turn == 0 else pltpu.roll(window, step + halo - turn, 0)
            for j in range(turn, reach, 8):
                total = total + taps_ref[reach - 1 - j : reach - j, column] * shifted[j - turn : j - turn + step]
        here = pl.ds(start, step)
        gate_sig = jax.nn.sigmoid(r["gate"][here, column].astype(f32))
        moved = total * gate_sig
        outs[4][here, column] = moved.astype(bf16)
        outs[5][here, column] = (moved * r["value"][here, column].astype(f32) * (1.0 - gate_sig)).astype(bf16)
        return carry

    turns = (tokens // step - 1) * strips
    line = [(0, 0), (1, 0), (2, 0), (3, 0), (0, 1), (1, 1), (2, 1), (3, 1)]
    tasks = [(*g, 1) for g in line[5:]]
    for j in range(2, levels + 1):
        tasks += [(*g, j) for g in line]
    tasks.sort(key=lambda x: line.index(x[:2]) + 3 * x[2])
    cuts = len(tasks) - 2
    marks = [turns * i // cuts for i in range(cuts + 1)]
    for i, task in enumerate(tasks):
        if i == cuts:
            halo_send.wait_recv()
            tail_rows = beyond[...]
            extended[pl.ds(tokens, halo), :] = jnp.where(me == group - 1, jnp.zeros_like(tail_rows), tail_rows)
            lax.fori_loop(turns, turns + strips, convolve, 0)
            stores[4].start()
            stores[5].start()
        fold(*task)
        if i < cuts:
            lax.fori_loop(marks[i], marks[i + 1], convolve, 0)
    stores[3].start()
    for s in [me] + sp_peers:
        to_far(s).wait_send()
        to_near(s).wait_send()
        onward(s).wait_send()
        for h in range(2):
            part_near(s, 0, h).wait_send()
            part_near(s, 1, h).wait_send()
            part_far(s, h).wait_send()
    for s in sp_peers:
        swap(s).wait_send()
        to_home(s, 0).wait_send()
        to_home(s, 1).wait_send()
    for c in small + terms:
        c.wait_send()
    for h in range(2):
        wide_x(h).wait_send()
        for b in range(2):
            wide_far(b, h).wait_send()
            wide_near(b, h).wait_send()
            wide_on(b, h).wait_send()
    halo_send.wait_send()
    act_send.wait_send()
    for g in range(2 * narrow):
        for j in range(levels):
            trade(g, j).wait_send()
    for c in stores:
        c.wait()


def whole_pass(*args):
    group, narrow = lax.axis_size("sp"), lax.axis_size("tp")
    ids, weight, cot, conv, gain, rows_in, gate_w, up_w, down_w, proj_w, taps, value, gate = args
    tokens, width = cot.shape
    slots, model = rows_in.shape
    hidden = down_w.shape[0]
    cap = slots // group
    pairs = group // 2
    sub = width // group
    halo = -(-(taps.shape[0] - 1) // 8) * 8
    f32, bf16 = jnp.float32, jnp.bfloat16
    dma = pltpu.SemaphoreType.DMA
    rows = (slots, width)
    tile = (tokens, width)
    results = [
        ((model, hidden), bf16),
        ((model, hidden), bf16),
        ((hidden, model), bf16),
        ((sub, model), f32),
        (tile, bf16),
        (tile, bf16),
    ]
    scratch = dict(
        ids=VMEM(ids.shape, ids.dtype),
        weight=VMEM(weight.shape, weight.dtype),
        cot=VMEM(tile, bf16),
        conv=VMEM(tile, bf16),
        gain=VMEM(gain.shape, f32),
        pair_w=VMEM((model, 2 * hidden), bf16),
        down=VMEM(down_w.shape, bf16),
        down_t=VMEM((model, hidden), bf16),
        pair_t=VMEM((2 * hidden, model), bf16),
        proj=VMEM(proj_w.shape, bf16),
        taps=VMEM(taps.shape, f32),
        value=VMEM(tile, bf16),
        gate=VMEM(tile, bf16),
        out=VMEM(rows, bf16),
        cot_rows=VMEM((slots, model), bf16),
        act=VMEM((slots, hidden), bf16),
        up_slope=VMEM((slots, hidden), f32),
        gate_slope=VMEM((slots, hidden), f32),
        delta=VMEM((slots, 2 * hidden), bf16),
        part=VMEM((slots, model), bf16),
        pair_buf=VMEM((2,) + rows, bf16),
        far_out=VMEM(rows, bf16),
        far_in=VMEM(rows, bf16),
        done=VMEM(rows, bf16),
        home=VMEM(rows, bf16),
        stat=VMEM((8, tokens), f32),
        stats=VMEM((narrow, 8, tokens), f32),
        term=VMEM((8, tokens), f32),
        terms=VMEM((narrow - 1, 8, tokens), f32),
        mix_both=VMEM((2 * tokens, model), bf16),
        product=VMEM((group, sub, width // 2), f32),
        kept=VMEM((2 * narrow, pairs // 2, sub, width // 2), f32),
        own_sum=VMEM((sub, model), f32),
        extended=VMEM((tokens + halo, width), f32),
        beyond=VMEM((halo, width), f32),
        conv_act=VMEM((2 * tokens, width), bf16),
        hat=VMEM(tile, f32),
        slope=VMEM(tile, f32),
        dev=VMEM((tokens, 1), f32),
        gate_stage=VMEM((model, hidden), bf16),
        up_stage=VMEM((model, hidden), bf16),
        down_stage=VMEM((hidden, model), bf16),
        value_stage=VMEM(tile, bf16),
        grad_stage=VMEM(tile, bf16),
        l_s=dma((len(args),)),
        o_s=dma((len(results),)),
        e_s=dma((2,)),
        e_r=dma((2,)),
    )
    scratch["in"] = VMEM(rows_in.shape, bf16)
    levels = pairs.bit_length() - 1
    for j in range(levels):
        held = VMEM((2 * narrow, pairs >> (j + 1), sub, width // 2), bf16)
        scratch["go%d" % j] = scratch["come%d" % j] = held
    for n in ("a", "n", "f", "m"):
        scratch[n + "_s"] = scratch[n + "_r"] = dma((group,))
    for n in ("pf", "h"):
        scratch[n + "_s"] = scratch[n + "_r"] = dma((group, 2))
    scratch["pn_s"] = scratch["pn_r"] = dma((group, 4))
    for n in ("t", "u"):
        scratch[n + "_s"] = scratch[n + "_r"] = dma((narrow - 1,))
    for n in ("wn", "wf", "wm"):
        scratch[n + "_s"] = scratch[n + "_r"] = dma((2, 2))
    scratch["x_s"] = scratch["x_r"] = dma((2,))
    scratch["y_s"] = scratch["y_r"] = dma((2 * narrow, levels))

    def body(*refs):
        whole_kernel(group, narrow, cap, len(args), len(results), tuple(scratch), *refs)

    return pl.pallas_call(
        body,
        name="whole_kernel",
        out_shape=tuple(jax.ShapeDtypeStruct(*x) for x in results),
        in_specs=[pl.BlockSpec(memory_space=pltpu.HBM)] * len(args),
        out_specs=[pl.BlockSpec(memory_space=pl.ANY)] * len(results),
        scratch_shapes=list(scratch.values()),
        compiler_params=pltpu.CompilerParams(
            collective_id=0, has_side_effects=True, vmem_limit_bytes=48 * 1024 * 1024
        ),
    )(*[pltpu.with_memory_space_constraint(x, pltpu.HBM) for x in args])


def emit_kernel(count, *refs):
    sems = refs[-1]
    copies = [pltpu.make_async_copy(refs[k], refs[count + k], sems.at[k]) for k in range(count)]
    for c in copies:
        c.start()
    for c in copies:
        c.wait()


def emit(*results):
    return pl.pallas_call(
        functools.partial(emit_kernel, len(results)),
        name="emit",
        out_shape=tuple(jax.ShapeDtypeStruct(x.shape, x.dtype) for x in results),
        in_specs=[pl.BlockSpec(memory_space=pl.ANY)] * len(results),
        out_specs=[pl.BlockSpec(memory_space=pltpu.HBM)] * len(results),
        scratch_shapes=[pltpu.SemaphoreType.DMA((len(results),))],
        compiler_params=pltpu.CompilerParams(vmem_limit_bytes=1024 * 1024),
    )(*results)


def per_device(
    cot_out,
    route_ids,
    route_weight,
    expert_inputs,
    w_gate,
    w_up,
    w_down,
    w_proj,
    conv_out,
    channel_norm_gain,
    taps,
    value_pre,
    gate_pre,
):
    group_size = lax.axis_size("sp")
    rows_in = expert_inputs[0]
    slot_rows, model_width = rows_in.shape
    capacity = slot_rows // group_size
    fitted = -(-capacity // 16) * 16
    if fitted != capacity:
        rows_in = rows_in.reshape(group_size, capacity, model_width)
        rows_in = jnp.pad(rows_in, ((0, 0), (0, fitted - capacity), (0, 0)))
        rows_in = rows_in.reshape(group_size * fitted, model_width)
    grad_gate_part, grad_up_part, grad_down, grad_proj, grad_value, grad_gate = emit(
        *whole_pass(
        route_ids.T,
        route_weight.T,
        cot_out,
        conv_out,
        channel_norm_gain[None, :],
        rows_in,
        w_gate[0],
        w_up[0],
        w_down[0],
        w_proj,
        taps,
        value_pre,
        gate_pre,
        )
    )
    return (
        grad_gate_part[None],
        grad_up_part[None],
        grad_down[None],
        grad_proj,
        grad_value,
        grad_gate,
    )


def solution(mesh):
    return jax.shard_map(
        per_device,
        mesh=mesh,
        in_specs=(
            P("sp", "tp"),
            P("sp", None),
            P("sp", None),
            P("sp", None, None),
            P("sp", None, "tp"),
            P("sp", None, "tp"),
            P("sp", "tp", None),
            P("tp", None),
            P("sp", "tp"),
            P("tp"),
            P(None, "tp"),
            P("sp", "tp"),
            P("sp", "tp"),
        ),
        out_specs=(
            P("sp", None, "tp"),
            P("sp", None, "tp"),
            P("sp", "tp", None),
            P(("tp", "sp"), None),
            P("sp", "tp"),
            P("sp", "tp"),
        ),
        check_vma=False,
    )
```
